32 devices in a mesh: grp: 2 (over y), sp: 8 (over z, core), tp: 2 (over x).
Axes of the slice: x: 2, y: 2, z: 4, core: 2. Of those that a mesh axis runs over, the one named last changes fastest.
Arguments:
- resid: bfloat16 [3072, 2048], P(('grp', 'sp', 'tp')), parts along dimension 0, may hold values from -6 to 6
- queries: bfloat16 [3072, 1024], P(('grp', 'sp'), 'tp'), parts along dimension 0, may hold values from -64 to 64
- keys: bfloat16 [3072, 256], P(('grp', 'sp'), 'tp'), parts along dimension 0, may hold values from -64 to 64
- values: bfloat16 [3072, 256], P(('grp', 'sp'), 'tp'), parts along dimension 0, may hold values from -6 to 6
- doc_ids: int32 [3072], P(('grp', 'sp')), parts along dimension 0, may hold values from 0 to 3, never falling along the last dimension, each value on 1 to 768 neighbouring positions
- sink_logits: float32 [16], P('tp'), may hold values from 2 to 6
- out_proj: bfloat16 [1024, 2048], P('tp'), may hold values from -1.5 to 1.5
- norm1_gain: float32 [2048], replicated, may hold values from 0.1 to 1.9
- norm1_bias: float32 [2048], replicated, may hold values from -1.8 to 1.8
- route_ids: int32 [3072, 2], P(('grp', 'sp', 'tp')), parts along dimension 0, may hold values from 0 to 7, all different within a row; in each aligned block of 96 rows (0 to 95, 96 to 191, ...) at most 30 rows name the same one
- route_weights: float32 [3072, 2], P(('grp', 'sp', 'tp')), parts along dimension 0, may hold values from 0.25 to 1
- expert_gate: bfloat16 [8, 2048, 3072], P('sp', None, 'tp'), may hold values from -0.125 to 0.125
- expert_up: bfloat16 [8, 2048, 3072], P('sp', None, 'tp'), may hold values from -0.125 to 0.125
- expert_down: bfloat16 [8, 3072, 2048], P('sp', 'tp'), may hold values from -0.109375 to 0.109375
- norm2_gain: float32 [2048], replicated, may hold values from 0.1 to 1.9
- norm2_bias: float32 [2048], replicated, may hold values from -1.8 to 1.8
Outputs:
- mixed: bfloat16 [3072, 2048], P(('grp', 'sp', 'tp')), parts along dimension 0
The draws below stay inside these ranges and needn't reach their ends.
There are 2 independent parts, one for each index of `grp`. The reference program is written for one: setup_inputs(seed, part) draws one part's arguments, and reference() takes and returns one part's arrays. A program takes and returns all parts, laid end to end along the dimension named above; an argument that names none is the same for every part. Nothing has to cross between parts.
Inputs may be any that keep to these rules, and one draw needn't show every extreme that they name: `route_ids`: among the rows of one device (aligned blocks of 96 tokens) no expert is named more than 30 times, a bound that some block reaches; a token's 2 experts differ.
All inputs are finite; a program needn't handle non-finite values.
Results may differ from the reference program's by a relative error of at most 0.012.
Values may be sent and summed in bfloat16 or wider, within the bound.
A program may use at most 64 MiB of HBM per device.

```python
import math
import jax
import jax.numpy as jnp
import numpy as np
from jax import lax

D = 2048
HEADS = 16
KV_HEADS = 4
HEAD_DIM = 64
ATT_WIDTH = 1024
FF = 3072
TOPK = 2
WINDOW = 128
TOK_DEV = 192
TOK_SUB = 96
TOKENS = 1536
EXPERTS = 8
CAP = 30
DOCS = 4
DOC_MOST = 768
N_TP = 2


def draw_keys(key, part):
    noise = jnp.clip(jax.random.normal(jax.random.fold_in(key, 1), (TOKENS, KV_HEADS, HEAD_DIM), jnp.float32), -6.0, 6.0)
    return noise.reshape(TOKENS, KV_HEADS * HEAD_DIM).astype(jnp.bfloat16)


def draw_queries(key, part):
    noise = jnp.clip(jax.random.normal(jax.random.fold_in(key, 2), (TOKENS, HEADS, HEAD_DIM), jnp.float32), -6.0, 6.0)
    return noise.reshape(TOKENS, HEADS * HEAD_DIM).astype(jnp.bfloat16)


def block_levels(key, dims, cuts, smallest, high):
    gain, own = 1.0, jax.random.fold_in(key, 6)
    for dim, parts in cuts:
        draws = jnp.exp(jax.random.uniform(jax.random.fold_in(own, dim), (parts,), jnp.float32, smallest / len(cuts), high / len(cuts)))
        gain = gain * jnp.repeat(draws, dims[dim] // parts).reshape([-1 if axis == dim else 1 for axis in range(len(dims))])
    return gain


def profile(number_of, total, most, slope):
    weights = [(1 << 20) // math.isqrt(standing ** slope) + 1 for standing in range(2, number_of + 1)]
    surplus, holding = total - most - (number_of - 1), [1] * (number_of - 1)
    while surplus > 0:
        free = [i for i in range(number_of - 1) if holding[i] < most]
        whole, budget = sum([weights[i] for i in free]), surplus
        for i in free:
            extra = min(most - holding[i], max(1, budget * weights[i] // whole), surplus)
            holding[i] = holding[i] + extra
            surplus = surplus - extra
    return np.array([most] + holding)


def uneven(rng, amount, total, most, lean):
    if amount == 2:
        one = jax.random.randint(rng, (), max(1, total - most), min(most, total - 1) + 1)
        return jnp.stack([one, total - one])
    lengths = jnp.asarray(profile(amount, total, most, lean), jnp.int32)
    pairs = (amount - 1) // 2
    source_of, sink = lengths[1:1 + 2 * pairs:2], lengths[2:2 + 2 * pairs:2]
    room = jnp.minimum(source_of - 1, most - sink)
    moved = jax.random.randint(jax.random.fold_in(rng, 1), (pairs,), 0, 1 << 20) % (room + 1)
    lengths = lengths.at[1:1 + 2 * pairs:2].set(source_of - moved).at[2:2 + 2 * pairs:2].set(sink + moved)
    return lengths[jax.random.permutation(jax.random.fold_in(rng, 2), amount)]


def assign_block(rng, own, number, rows, count, top, most, skew):
    sequence = jax.random.permutation(rng, count)
    packed, usual = load_shares(count, rows * top, most, skew, True), load_shares(count, rows * top, most, skew, False)
    places = jnp.arange(count)

    def named(sizes, rotation):
        used = int((sizes > 0).sum())
        fixed = max(1, used // 4)
        moved = fixed + (places - fixed + rotation * (used - fixed)) % max(1, count - fixed)
        return jnp.zeros((count,), jnp.int32).at[sequence[jnp.where(places < fixed, places, moved)]].set(jnp.asarray(sizes, jnp.int32))

    sizes = jnp.where(number % 4 == 0, named(packed, number // 4), named(usual, number - number // 4 - 1))
    mixed = jax.random.permutation(jax.random.fold_in(own, 3), count)
    donor, sink = mixed[0:count // 2 * 2:2], mixed[1:count // 2 * 2:2]
    room = jnp.minimum(sizes[donor] - 1, most - sizes[sink]) // 2
    room = jnp.where((donor == sequence[0]) | (sink == sequence[0]) | (sizes[sink] == 0), 0, jnp.maximum(room, 0))
    moved = jax.random.randint(jax.random.fold_in(own, 4), (count // 2,), 0, 1 << 20) % (room + 1)
    sizes = sizes.at[donor].add(-moved).at[sink].add(moved)
    labels = jnp.searchsorted(jnp.cumsum(sizes), jnp.arange(rows * top), side="right").astype(jnp.int32)
    grid = labels.reshape(top, rows).T
    grid = grid[jax.random.permutation(jax.random.fold_in(own, 1), rows)]
    rotation = jax.random.randint(jax.random.fold_in(own, 2), (rows, 1), 0, top)
    return jnp.take_along_axis(grid, (jnp.arange(top)[None, :] + rotation) % top, axis=1)


def load_shares(amount, total, limit, skew, full):
    weights = [(1 << 20) // math.isqrt(grade ** skew) + 1 for grade in range(1, amount + 1)]
    largest = limit if full else min(limit, max(-(-total // amount), total * weights[0] // sum(weights)))
    least = 1 if total - largest >= amount - 1 else 0
    given, rest = [largest] + [least] * (amount - 1), total - largest - least * (amount - 1)
    while rest > 0:
        free = [i for i in range(1, amount) if given[i] < largest] or [i for i in range(1, amount) if given[i] < limit]
        mass, budget = sum([weights[i] for i in free]), rest
        for i in free:
            extra = min(limit - given[i], max(1, budget * weights[i] // mass), rest)
            given[i] = given[i] + extra
            rest = rest - extra
    return np.array(given)


def normal_values(own_key, extent, spread, most, shards=(), held_as=jnp.bfloat16):
    values = jax.random.normal(own_key, extent, jnp.float32) * spread
    if len(shards) > 0:
        values = block_levels(own_key, extent, shards, -0.22, 0.18) * values
    return jnp.clip(values, min=-most, max=most).astype(held_as)


def setup_inputs(seed: int = 0, part: int = 0) -> dict:
    seeds = jax.random.split(jax.random.key(seed), 17)
    part_keys = jax.random.split(jax.random.fold_in(seeds[16], part), 17)
    resid = normal_values(part_keys[0], (TOKENS, D), 1.0, 6.0, ((0, 16),))
    queries = draw_queries(jax.random.fold_in(jax.random.fold_in(seeds[16], part), 71), part)
    keys = draw_keys(jax.random.fold_in(jax.random.fold_in(seeds[16], part), 71), part)
    values = normal_values(part_keys[3], (TOKENS, KV_HEADS * HEAD_DIM), 1.0, 6.0, ((0, 8), (1, 2)))
    doc_ids = jnp.searchsorted(jnp.cumsum(uneven(part_keys[4], DOCS, TOKENS, DOC_MOST, 2)), jnp.arange(TOKENS), side="right").astype(jnp.int32)
    sink_logits = jnp.clip(2.0 + 4.0 * jax.random.uniform(seeds[5], (HEADS,), jnp.float32) ** block_levels(seeds[5], (HEADS,), ((0, 2),), -0.2, 0.2), 2.0, 6.0)
    out_proj = normal_values(seeds[6], (ATT_WIDTH, D), (HEAD_DIM // 4) ** -0.5, 1.5, ((0, 2),))
    norm1_gain = jnp.clip(1.0 + 0.18 * jax.random.normal(seeds[7], (D,), jnp.float32), 0.1, 1.9)
    norm1_bias = normal_values(seeds[8], (D,), 0.3, 1.8, (), jnp.float32)
    route_ids_keys = jax.random.split(jax.random.fold_in(part_keys[9], 1), TOKENS // TOK_SUB)
    route_ids_turns = jax.random.permutation(jax.random.fold_in(part_keys[9], 3), TOKENS // TOK_SUB)
    route_ids = jax.vmap(lambda own, number: assign_block(jax.random.fold_in(part_keys[9], 2), own, number, TOK_SUB, EXPERTS, TOPK, CAP, 1))(route_ids_keys, route_ids_turns).reshape((TOKENS, TOPK))
    route_weights = jnp.clip(0.25 + 0.75 * jax.random.uniform(part_keys[10], (TOKENS, TOPK), jnp.float32) ** block_levels(part_keys[10], (TOKENS, TOPK), ((0, 16),), -0.2, 0.2), 0.25, 1.0)
    expert_gate = normal_values(seeds[11], (EXPERTS, D, FF), D ** -0.5, 0.125, ((0, 8), (2, 2)))
    expert_up = normal_values(seeds[12], (EXPERTS, D, FF), D ** -0.5, 0.125, ((0, 8), (2, 2)))
    expert_down = normal_values(seeds[13], (EXPERTS, FF, D), FF ** -0.5, 0.109375, ((0, 8), (1, 2)))
    norm2_gain = jnp.clip(1.0 + 0.18 * jax.random.normal(seeds[14], (D,), jnp.float32), 0.1, 1.9)
    norm2_bias = normal_values(seeds[15], (D,), 0.3, 1.8, (), jnp.float32)
    return {"resid": resid, "queries": queries, "keys": keys, "values": values, "doc_ids": doc_ids, "sink_logits": sink_logits, "out_proj": out_proj, "norm1_gain": norm1_gain, "norm1_bias": norm1_bias, "route_ids": route_ids, "route_weights": route_weights, "expert_gate": expert_gate, "expert_up": expert_up, "expert_down": expert_down, "norm2_gain": norm2_gain, "norm2_bias": norm2_bias}


norm_epsilon = 1e-05
residual_scale = 1.4142135623730951
masked_score = -1e+30

def layer_norm(values, gain_vec, bias_vec):
    mean_val = lax.optimization_barrier(jnp.mean(values, -1, keepdims=True))
    centred = values - mean_val
    variance = lax.optimization_barrier(jnp.mean(centred * centred, -1, keepdims=True))
    return centred * lax.rsqrt(variance + norm_epsilon) * gain_vec + bias_vec

def attention(queries, keys, values, doc_ids, sink_logits):
    groups = HEADS // KV_HEADS
    block = TOK_DEV
    nblocks = TOKENS // block
    reach = block + 2 * WINDOW
    pad_keys = jnp.pad(keys.reshape(TOKENS, KV_HEADS, HEAD_DIM), ((WINDOW, WINDOW), (0, 0), (0, 0)))
    pad_values = jnp.pad(values.reshape(TOKENS, KV_HEADS, HEAD_DIM), ((WINDOW, WINDOW), (0, 0), (0, 0)))
    pad_docs = jnp.pad(doc_ids.astype(jnp.int32), (WINDOW, WINDOW))
    sink_table = sink_logits.astype(jnp.float32).reshape(KV_HEADS, groups, 1, 1)

    def one_block(index):
        start = index * block
        query_blk = lax.dynamic_slice_in_dim(queries, start, block, 0).reshape(block, KV_HEADS, groups, HEAD_DIM)
        key_blk = lax.dynamic_slice_in_dim(pad_keys, start, reach, 0)
        value_blk = lax.dynamic_slice_in_dim(pad_values, start, reach, 0)
        query_docs = lax.dynamic_slice_in_dim(doc_ids.astype(jnp.int32), start, block, 0)
        key_docs = lax.dynamic_slice_in_dim(pad_docs, start, reach, 0)
        query_pos = start + jnp.arange(block, dtype=jnp.int32)
        key_pos = start - WINDOW + jnp.arange(reach, dtype=jnp.int32)
        allowed = (key_pos[None, :] >= 0) & (key_pos[None, :] < TOKENS)
        allowed = allowed & (jnp.abs(query_pos[:, None] - key_pos[None, :]) <= WINDOW)
        allowed = allowed & (query_docs[:, None] == key_docs[None, :])
        scores = jnp.einsum('qkgd,jkd->kgqj', query_blk.astype(jnp.float32), key_blk.astype(jnp.float32))
        scores = jnp.where(allowed, scores * HEAD_DIM ** (-0.5), masked_score)
        top_score = jnp.maximum(lax.optimization_barrier(jnp.max(scores, -1, keepdims=True)), sink_table)
        raised = jnp.where(allowed, jnp.exp(scores - top_score), 0.0)
        denominator = jnp.exp(sink_table - top_score) + lax.optimization_barrier(jnp.sum(raised, -1, keepdims=True))
        weights = (raised / denominator).astype(jnp.bfloat16)
        result = jnp.einsum('kgqj,jkd->qkgd', weights.astype(jnp.float32), value_blk.astype(jnp.float32))
        return result.astype(jnp.bfloat16).reshape(block, HEADS * HEAD_DIM)
    blocks = lax.map(one_block, jnp.arange(nblocks, dtype=jnp.int32))
    return blocks.reshape(TOKENS, HEADS * HEAD_DIM)

def experts_part(normed, route_ids, route_weights, expert_gate, expert_up, expert_down):
    nblocks = TOKENS // TOK_SUB
    slot_count = nblocks * CAP
    flat_ids = route_ids.reshape(nblocks, TOK_SUB * TOPK).astype(jnp.int32)
    one_hot = (flat_ids[:, :, None] == jnp.arange(EXPERTS, dtype=jnp.int32)[None, None, :]).astype(jnp.int32)
    ranks = (jnp.cumsum(one_hot, axis=1) - 1).astype(jnp.int32)
    slot_rank = lax.optimization_barrier(jnp.sum(ranks * one_hot, axis=-1)).astype(jnp.int32)
    block_ids = jnp.arange(nblocks, dtype=jnp.int32)[:, None]
    targets = (flat_ids * slot_count + block_ids * CAP + slot_rank).reshape(-1).astype(jnp.int32)
    owners = (block_ids * TOK_SUB + jnp.arange(TOK_SUB * TOPK, dtype=jnp.int32)[None, :] // TOPK).reshape(-1).astype(jnp.int32)
    token_table = jnp.full((EXPERTS * slot_count,), TOKENS, jnp.int32).at[targets].set(owners).reshape(EXPERTS, slot_count)
    weight_table = jnp.zeros((EXPERTS * slot_count,), jnp.float32).at[targets].set(route_weights.reshape(-1).astype(jnp.float32)).reshape(EXPERTS, slot_count)
    padded = jnp.concatenate([normed, jnp.zeros((1, D), normed.dtype)], 0)
    hidden_cols = FF // N_TP

    def one_expert(total, inputs):
        gate_weight, up_weight, down_weight, token_rows, row_weights = inputs
        row_block = jnp.take(padded, token_rows, axis=0)
        gate_act = jnp.dot(row_block, gate_weight, preferred_element_type=jnp.float32)
        up_act = jnp.dot(row_block, up_weight, preferred_element_type=jnp.float32)
        hidden = (jax.nn.silu(gate_act) * up_act).astype(jnp.bfloat16)
        summed = jnp.zeros((slot_count, D), jnp.float32)
        for member in range(N_TP):
            piece_out = jnp.dot(hidden[:, member * hidden_cols:(member + 1) * hidden_cols], down_weight[member * hidden_cols:(member + 1) * hidden_cols], preferred_element_type=jnp.float32)
            summed = summed + lax.optimization_barrier(piece_out.astype(jnp.bfloat16)).astype(jnp.float32)
        expert_out = lax.optimization_barrier(summed.astype(jnp.bfloat16)).astype(jnp.float32)
        return (total.at[token_rows].add(row_weights[:, None] * expert_out), None)
    total, _ = lax.scan(one_expert, jnp.zeros((TOKENS + 1, D), jnp.float32), (expert_gate, expert_up, expert_down, token_table, weight_table))
    return total[:TOKENS]

def reference(resid, queries, keys, values, doc_ids, sink_logits, out_proj, norm1_gain, norm1_bias, route_ids, route_weights, expert_gate, expert_up, expert_down, norm2_gain, norm2_bias):
    attended = attention(queries, keys, values, doc_ids, sink_logits)
    head_cols = ATT_WIDTH // N_TP
    projected = jnp.zeros((TOKENS, D), jnp.float32)
    for member in range(N_TP):
        piece_out = jnp.dot(attended[:, member * head_cols:(member + 1) * head_cols], out_proj[member * head_cols:(member + 1) * head_cols], preferred_element_type=jnp.float32)
        projected = projected + lax.optimization_barrier(piece_out.astype(jnp.bfloat16)).astype(jnp.float32)
    projected = lax.optimization_barrier(projected.astype(jnp.bfloat16)).astype(jnp.float32)
    pre_norm = residual_scale * resid.astype(jnp.float32) + projected
    normed = layer_norm(pre_norm, norm1_gain, norm1_bias).astype(jnp.bfloat16)
    moe_sum = experts_part(normed, route_ids, route_weights, expert_gate, expert_up, expert_down)
    pre_final = residual_scale * normed.astype(jnp.float32) + moe_sum
    return layer_norm(pre_final, norm2_gain, norm2_bias).astype(jnp.bfloat16)
```

```python
import functools

import jax
import jax.numpy as jnp
from jax import lax
from jax.experimental import pallas as pl
from jax.experimental.pallas import tpu as pltpu
from jax.sharding import PartitionSpec as P

HEAD_DIM = 64
WINDOW = 128
MESH = pl.DeviceIdType.MESH
CHUNKS = 4
HEAD_TILE = 512


norm_epsilon = 1e-05
residual_scale = 1.4142135623730951
masked_score = -1e30


def layer_norm(values, gain_vec, bias_vec):
    mean_val = jnp.mean(values, -1, keepdims=True)
    centred = values - mean_val
    variance = jnp.mean(centred * centred, -1, keepdims=True)
    return centred * lax.rsqrt(variance + norm_epsilon) * gain_vec + bias_vec


def step_partner(step, sp_pos, count, back):
    chip, core = sp_pos // 2, sp_pos % 2
    half = count // 4
    side, place = chip // half, chip % half
    pair, flip = step // 2, step % 2
    if pair == 0:
        turn, cross = 0, False
    elif pair <= half:
        turn, cross = pair - 1, True
    else:
        turn, cross = pair - half, False
    target_side = 1 - side if cross else side
    move = half - turn if back else turn
    target = target_side * half + (place + move) % half
    return target * 2 + (core + flip) % 2


def chain_of_four(sp_pos):
    chip, core = sp_pos // 2, sp_pos % 2
    inner = chip * (3 - chip) // 2
    return chip, core, inner, chip + 1 - 2 * (chip % 2)


def target_of(step, sp_pos, count):
    if count != 8:
        return step_partner(step, sp_pos, count, False), step
    chip, core, inner, near = chain_of_four(sp_pos)
    pair, flip = step // 2, step % 2
    to = (chip, (chip + 2) % 4, near, 3 - chip)[pair]
    slot = step if pair < 2 else 6 - 2 * inner + flip
    return to * 2 + (core + flip) % 2, slot


def source_of(slot, sp_pos, count):
    if count != 8:
        return step_partner(slot, sp_pos, count, True)
    chip, core, inner, near = chain_of_four(sp_pos)
    pair, flip = slot // 2, slot % 2
    far = 3 - chip
    of = (
        chip,
        (chip + 2) % 4,
        inner * far + (1 - inner) * near,
        inner * near + (1 - inner) * far,
    )[pair]
    return of * 2 + (core + flip) % 2


def work_order(count):
    if count == 8:
        return [
            ("F", (0,)),
            ("F", (1,)),
            ("F", (2,)),
            ("U", (0, 1,)),
            ("D", (0, 1,)),
            ("X", (0,)),
            ("U", (2,)),
            ("F", (3,)),
            ("D", (2,)),
            ("X", (2,)),
            ("U", (3,)),
            ("F", (4,)),
            ("D", (3,)),
            ("X", (3,)),
            ("G", (2,)),
            ("F", (5,)),
            ("U", (4,)),
            ("F", (6,)),
            ("D", (4,)),
            ("X", (4,)),
            ("G", (3,)),
            ("U", (5,)),
            ("F", (7,)),
            ("D", (5,)),
            ("X", (5,)),
            ("G", (4,)),
            ("U", (6,)),
            ("D", (6,)),
            ("X", (6,)),
            ("G", (5,)),
            ("U", (7,)),
            ("D", (7,)),
            ("X", (7,)),
            ("X", (1,)),
            ("G", (6,)),
            ("G", (7,)),
            ("G", (0,)),
            ("G", (1,)),
        ]
    chunk = count // CHUNKS
    groups = [tuple(range(c * chunk, (c + 1) * chunk)) for c in range(CHUNKS)]
    order = [("F", groups[0])]
    for c, group in enumerate(groups):
        order.append(("U", group))
        if c + 1 < CHUNKS:
            order.append(("F", groups[c + 1]))
        order += [("D", group), ("X", group)]
        if c > 0:
            order.append(("G", groups[c - 1]))
    return order + [("G", groups[-1])]


def head_copy(d, i, t, tps, head_part, head_peer, head_send, head_recv):
    cols = pl.ds(pl.multiple_of(i * HEAD_TILE, HEAD_TILE), HEAD_TILE)
    return pltpu.make_async_remote_copy(
        src_ref=head_part.at[d, :, cols],
        dst_ref=head_peer.at[d, :, cols],
        send_sem=head_send.at[d, i],
        recv_sem=head_recv.at[d, i],
        device_id={"tp": (t + d) % tps},
        device_id_type=MESH,
    )


def attend(
    count,
    tps,
    queries_ref,
    keys_ref,
    values_ref,
    docs_ref,
    sink_ref,
    proj_w,
    key_pad,
    value_pad,
    doc_side,
    doc_rows,
    doc_cols,
    attended,
    head_part,
    head_peer,
    halo_send,
    halo_recv,
    head_send,
    head_recv,
    barrier,
    kv_copies,
    query_copies,
    proj_copy,
):
    me, t = lax.axis_index("sp"), lax.axis_index("tp")
    tok_dev, tok_sub = queries_ref.shape[0], attended.shape[0]
    local_kv = keys_ref.shape[1] // HEAD_DIM
    heads = queries_ref.shape[1] // HEAD_DIM
    groups = heads // local_kv
    reach = doc_rows.shape[2]
    end = WINDOW + tok_dev
    rest = key_pad.shape[0] - end - WINDOW
    for copy in kv_copies:
        copy.wait()
    pl.semaphore_wait(barrier, count - 1 + tps - 1)
    copies = []
    for side in range(2):
        start, place = (tok_dev - WINDOW, 0) if side == 0 else (0, end)
        to = (me + 1) % count if side == 0 else (me + count - 1) % count
        pairs = (
            (keys_ref.at[pl.ds(start, WINDOW)], key_pad.at[pl.ds(place, WINDOW)]),
            (values_ref.at[pl.ds(start, WINDOW)], value_pad.at[pl.ds(place, WINDOW)]),
            (docs_ref, doc_side.at[side]),
        )
        for i, (own, pad) in enumerate(pairs):
            copies.append(
                pltpu.make_async_remote_copy(
                    src_ref=own,
                    dst_ref=pad,
                    send_sem=halo_send.at[2 * i + side],
                    recv_sem=halo_recv.at[2 * i + side],
                    device_id={"sp": to},
                    device_id_type=MESH,
                )
            )
    for copy in copies:
        copy.start()
    for pad, own in ((key_pad, keys_ref), (value_pad, values_ref)):
        pad[WINDOW:end] = own[...]
        if rest:
            pad[end + WINDOW :] = jnp.zeros((rest, pad.shape[1]), pad.dtype)
    doc_cols[...] = jnp.transpose(jnp.broadcast_to(docs_ref[...], (128, tok_dev)))
    for copy in query_copies:
        copy.wait()
    for copy in copies:
        copy.wait_recv()
    doc_row = jnp.concatenate(
        [doc_side[0][:, tok_dev - WINDOW :], docs_ref[...], doc_side[1][:, :WINDOW]]
        + ([jnp.zeros((1, rest), jnp.int32)] if rest else []),
        1,
    )
    for j in range(tps):
        doc_rows[j] = doc_row[:, j * tok_sub : j * tok_sub + reach]

    tile = HEAD_TILE
    width = proj_w.shape[1]
    for d in list(range(1, tps)) + [0]:
        block = (t + d) % tps
        base = pl.multiple_of(block * tok_sub, 16)
        key_block = key_pad[pl.ds(base, reach), :].astype(jnp.float32)
        value_block = value_pad[pl.ds(base, reach), :].astype(jnp.float32)
        key_docs = doc_rows[block]
        query_docs = doc_cols[pl.ds(base, tok_sub), 0:1]
        row = lax.broadcasted_iota(jnp.int32, (tok_sub, reach), 0)
        col = lax.broadcasted_iota(jnp.int32, (tok_sub, reach), 1)
        position = me * tok_dev + base - WINDOW + col
        allowed = (position >= 0) & (position < count * tok_dev)
        allowed = allowed & (col >= row) & (col <= row + 2 * WINDOW)
        allowed = allowed & (query_docs == key_docs)
        blank = jnp.zeros((reach, HEAD_DIM), jnp.float32)
        for g in range(local_kv):
            span = slice(g * HEAD_DIM, (g + 1) * HEAD_DIM)
            sides = []
            for block in (key_block, value_block):
                piece = block[:, span]
                sides.append(
                    [
                        jnp.concatenate([piece, blank], 1).astype(jnp.bfloat16),
                        jnp.concatenate([blank, piece], 1).astype(jnp.bfloat16),
                    ]
                )
            for pair in range(groups // 2):
                lane = (g * groups + 2 * pair) * HEAD_DIM
                query = queries_ref[pl.ds(base, tok_sub), lane : lane + 2 * HEAD_DIM]
                result = jnp.zeros((tok_sub, 2 * HEAD_DIM), jnp.float32)
                for parity in range(2):
                    head = g * groups + 2 * pair + parity
                    sink = sink_ref[:, head : head + 1]
                    scores = lax.dot_general(
                        query,
                        sides[0][parity],
                        (((1,), (1,)), ((), ())),
                        preferred_element_type=jnp.float32,
                    )
                    scores = jnp.where(allowed, scores * HEAD_DIM ** (-0.5), masked_score)
                    top = jnp.maximum(jnp.max(scores, -1, keepdims=True), sink)
                    raised = jnp.where(allowed, jnp.exp(scores - top), 0.0)
                    total = jnp.exp(sink - top) + jnp.sum(raised, -1, keepdims=True)
                    weights = (raised / total).astype(jnp.bfloat16)
                    result = result + jnp.dot(
                        weights, sides[1][parity], preferred_element_type=jnp.float32
                    )
                attended[:, lane : lane + 2 * HEAD_DIM] = result.astype(jnp.bfloat16)
        if d == 1 or tps == 1:
            proj_copy.wait()

        def project(i, carry):
            cols = pl.ds(pl.multiple_of(i * tile, tile), tile)
            head_part[d, :, cols] = jnp.dot(
                attended[...], proj_w[:, cols], preferred_element_type=jnp.float32
            ).astype(jnp.bfloat16)
            if d:
                head_copy(d, i, t, tps, head_part, head_peer, head_send, head_recv).start()
            return carry

        lax.fori_loop(0, width // tile, project, 0)
    for copy in copies:
        copy.wait_send()


def layer_kernel(
    experts,
    tps,
    order,
    queries_hbm,
    keys_hbm,
    values_hbm,
    docs_hbm,
    sink_hbm,
    gain1_hbm,
    bias1_hbm,
    ids_hbm,
    mix_hbm,
    gain_hbm,
    bias_hbm,
    resid_hbm,
    proj_hbm,
    gate_hbm,
    up_hbm,
    down_hbm,
    out_ref,
    queries_ref,
    keys_ref,
    values_ref,
    docs_ref,
    sink_ref,
    gain1_ref,
    bias1_ref,
    ids_ref,
    mix_ref,
    gain_ref,
    bias_ref,
    resid_ref,
    proj_w,
    key_pad,
    value_pad,
    doc_side,
    doc_rows,
    doc_cols,
    attended,
    head_part,
    head_peer,
    pre_ref,
    normed_ref,
    assign_ref,
    combine_ref,
    outgoing,
    rows,
    gate_w,
    up_w,
    down_w,
    hidden,
    part,
    peer,
    summed,
    returned,
    in_sem,
    disp_send,
    disp_recv,
    fwd_send,
    fwd_recv,
    part_send,
    part_recv,
    ret_send,
    ret_recv,
    halo_send,
    halo_recv,
    head_send,
    head_recv,
):
    me, t = lax.axis_index("sp"), lax.axis_index("tp")
    _, capacity, width = outgoing.shape
    toks = normed_ref.shape[0]

    barrier = pltpu.get_barrier_semaphore()
    for d in range(1, experts):
        pl.semaphore_signal(
            barrier, inc=1, device_id={"sp": (me + d) % experts}, device_id_type=MESH
        )
    for d in range(1, tps):
        pl.semaphore_signal(barrier, inc=1, device_id={"tp": (t + d) % tps}, device_id_type=MESH)

    places = (
        (keys_hbm, keys_ref),
        (values_hbm, values_ref),
        (docs_hbm, docs_ref),
        (queries_hbm, queries_ref),
        (sink_hbm, sink_ref),
        (proj_hbm, proj_w),
        (ids_hbm, ids_ref),
        (mix_hbm, mix_ref),
        (resid_hbm, resid_ref),
        (gain1_hbm, gain1_ref),
        (bias1_hbm, bias1_ref),
        (gain_hbm, gain_ref),
        (bias_hbm, bias_ref),
        (gate_hbm.at[0], gate_w),
        (up_hbm.at[0], up_w),
        (down_hbm.at[0], down_w),
    )
    loads = [
        pltpu.make_async_copy(source, place, in_sem.at[i])
        for i, (source, place) in enumerate(places)
    ]
    for load in loads:
        load.start()
    weight_loads = loads[13:]

    attend(
        experts,
        tps,
        queries_ref,
        keys_ref,
        values_ref,
        docs_ref,
        sink_ref,
        proj_w,
        key_pad,
        value_pad,
        doc_side,
        doc_rows,
        doc_cols,
        attended,
        head_part,
        head_peer,
        halo_send,
        halo_recv,
        head_send,
        head_recv,
        barrier,
        loads[:3],
        loads[3:5],
        loads[5],
    )
    for load in loads[6:13]:
        load.wait()
    lanes = experts * capacity
    top = ids_ref.shape[0]
    expert_iota = lax.broadcasted_iota(jnp.int32, (experts, toks), 0)
    upper = (
        lax.broadcasted_iota(jnp.int32, (toks, toks), 0)
        < lax.broadcasted_iota(jnp.int32, (toks, toks), 1)
    ).astype(jnp.float32).astype(jnp.bfloat16)
    before = jnp.zeros((experts, 1), jnp.float32)
    slot_iota = lax.broadcasted_iota(jnp.int32, (lanes, toks), 0)
    assign = jnp.zeros((lanes, toks), jnp.float32)
    combine = jnp.zeros((lanes, toks), jnp.float32)
    for k in range(top):
        own = ids_ref[k : k + 1, :]
        hot = (own == expert_iota).astype(jnp.float32)
        rank = before + jnp.dot(hot.astype(jnp.bfloat16), upper, preferred_element_type=jnp.float32)
        rank = jnp.sum(rank * hot, axis=0, keepdims=True).astype(jnp.int32)
        before = before + jnp.sum(hot, axis=1, keepdims=True)
        match = (own * capacity + rank == slot_iota).astype(jnp.float32)
        assign = assign + match
        combine = combine + match * mix_ref[k : k + 1, :]
    assign_ref[...] = assign.astype(jnp.bfloat16)
    high = combine.astype(jnp.bfloat16)
    combine_ref[0] = high
    combine_ref[1] = (combine - high.astype(jnp.float32)).astype(jnp.bfloat16)

    total = jnp.zeros((toks, 1), jnp.float32)
    for i in range(width // HEAD_TILE):
        cols = slice(i * HEAD_TILE, (i + 1) * HEAD_TILE)
        projected = head_part[0, :, cols].astype(jnp.float32)
        for d in range(1, tps):
            head_copy(d, i, t, tps, head_part, head_peer, head_send, head_recv).wait_recv()
            projected = projected + head_peer[d, :, cols].astype(jnp.float32)
        projected = projected.astype(jnp.bfloat16).astype(jnp.float32)
        pre_norm = residual_scale * resid_ref[:, cols].astype(jnp.float32) + projected
        pre_ref[:, cols] = pre_norm
        total = total + jnp.sum(pre_norm, -1, keepdims=True)
    centred = pre_ref[...] - total * (1.0 / width)
    variance = jnp.mean(centred * centred, -1, keepdims=True)
    normed = centred * lax.rsqrt(variance + norm_epsilon) * gain1_ref[...] + bias1_ref[...]
    normed_ref[...] = normed.astype(jnp.bfloat16)
    spread = jnp.dot(assign_ref[...], normed_ref[...], preferred_element_type=jnp.float32)
    outgoing[...] = spread.astype(jnp.bfloat16).reshape(experts, capacity, width)

    def dispatch(step):
        dst, slot = target_of(step, me, experts)
        return pltpu.make_async_remote_copy(
            src_ref=outgoing.at[dst],
            dst_ref=rows.at[slot, t],
            send_sem=disp_send.at[step],
            recv_sem=disp_recv.at[slot],
            device_id={"sp": dst},
            device_id_type=MESH,
        )

    def arrived(slot):
        return pltpu.make_async_remote_copy(
            src_ref=outgoing.at[slot],
            dst_ref=rows.at[slot, t],
            send_sem=disp_send.at[slot],
            recv_sem=disp_recv.at[slot],
            device_id={"sp": source_of(slot, me, experts)},
            device_id_type=MESH,
        )

    def forward(step, d):
        dst = (t + d) % tps
        return pltpu.make_async_remote_copy(
            src_ref=rows.at[step, t],
            dst_ref=rows.at[step, t],
            send_sem=fwd_send.at[step, d],
            recv_sem=fwd_recv.at[step, d],
            device_id={"tp": dst},
            device_id_type=MESH,
        )

    def share(step, d):
        dst = (t + d) % tps
        return pltpu.make_async_remote_copy(
            src_ref=part.at[step, dst],
            dst_ref=peer.at[step, d],
            send_sem=part_send.at[step, d],
            recv_sem=part_recv.at[step, d],
            device_id={"tp": dst},
            device_id_type=MESH,
        )

    def give_back(step):
        return pltpu.make_async_remote_copy(
            src_ref=summed.at[step],
            dst_ref=returned.at[me],
            send_sem=ret_send.at[step],
            recv_sem=ret_recv.at[me],
            device_id={"sp": source_of(step, me, experts)},
            device_id_type=MESH,
        )

    for step in range(1, experts):
        dispatch(step).start()
    rows[0, t] = outgoing[me]

    def send_on(step):
        if step > 0:
            arrived(step).wait_recv()
        for d in range(1, tps):
            forward(step, d).start()

    def finish(step):
        total = part[step, t].astype(jnp.float32)
        for d in range(1, tps):
            share(step, d).wait_recv()
            total = total + peer[step, d].astype(jnp.float32)
        if step == 0:
            returned[me] = total.astype(jnp.bfloat16)
        else:
            summed[step] = total.astype(jnp.bfloat16)
            give_back(step).start()

    tile = 512 if gate_w.shape[1] % 512 == 0 else 256
    hidden_width = gate_w.shape[1]

    def up_stage(k0, k1):
        m = (k1 - k0) * tps * capacity
        for step in range(k0, k1):
            for d in range(1, tps):
                forward(step, d).wait_recv()

        def up_tile(i, carry):
            cols = pl.ds(pl.multiple_of(i * tile, tile), tile)
            block = rows[k0:k1].reshape(m, width)
            gate = jnp.dot(block, gate_w[:, cols], preferred_element_type=jnp.float32)
            up = jnp.dot(block, up_w[:, cols], preferred_element_type=jnp.float32)
            hidden[:m, cols] = (gate / (1.0 + jnp.exp(-gate)) * up).astype(jnp.bfloat16)
            return carry

        lax.fori_loop(0, hidden_width // tile, up_tile, 0)

    def down_stage(k0, k1):
        m = (k1 - k0) * tps * capacity

        def down_tile(i, carry):
            cols = pl.ds(pl.multiple_of(i * tile, tile), tile)
            result = jnp.dot(hidden[:m], down_w[:, cols], preferred_element_type=jnp.float32)
            part[k0:k1, :, :, cols] = result.astype(jnp.bfloat16).reshape(
                k1 - k0, tps, capacity, tile
            )
            return carry

        lax.fori_loop(0, width // tile, down_tile, 0)

    waiting = {"U": weight_loads[:2], "D": weight_loads[2:]}
    for action, steps in order:
        for load in waiting.pop(action, ()):
            load.wait()
        with jax.named_scope(f"{action}{steps[0]}"):
            if action == "U":
                up_stage(steps[0], steps[-1] + 1)
            elif action == "D":
                down_stage(steps[0], steps[-1] + 1)
            else:
                for step in steps:
                    if action == "F":
                        send_on(step)
                    elif action == "G":
                        finish(step)
                    else:
                        for d in range(1, tps):
                            share(step, d).start()

    for d in range(1, experts):
        src = (me + d) % experts
        pltpu.make_async_remote_copy(
            src_ref=summed.at[d],
            dst_ref=returned.at[src],
            send_sem=ret_send.at[d],
            recv_sem=ret_recv.at[src],
            device_id={"sp": src},
            device_id_type=MESH,
        ).wait_recv()

    back = returned[...].reshape(lanes, width)
    across = (((0,), (0,)), ((), ()))
    moe_sum = lax.dot_general(combine_ref[0], back, across, preferred_element_type=jnp.float32)
    moe_sum = moe_sum + lax.dot_general(
        combine_ref[1], back, across, preferred_element_type=jnp.float32
    )
    pre_final = residual_scale * normed_ref[...].astype(jnp.float32) + moe_sum
    out_ref[...] = layer_norm(pre_final, gain_ref[...], bias_ref[...]).astype(jnp.bfloat16)

    for d in range(1, tps):
        for i in range(width // HEAD_TILE):
            head_copy(d, i, t, tps, head_part, head_peer, head_send, head_recv).wait_send()
    for step in range(experts):
        if step > 0:
            dispatch(step).wait_send()
            give_back(step).wait_send()
        for d in range(1, tps):
            forward(step, d).wait_send()
            share(step, d).wait_send()


def per_device(
    resid,
    queries,
    keys,
    values,
    doc_ids,
    sink_logits,
    out_proj,
    norm1_gain,
    norm1_bias,
    route_ids,
    route_weights,
    expert_gate,
    expert_up,
    expert_down,
    norm2_gain,
    norm2_bias,
):
    experts, tps = lax.axis_size("sp"), lax.axis_size("tp")
    toks, width = resid.shape
    tok_dev, kv_width = keys.shape
    need = 5 * toks // (2 * experts)
    capacity = -(-need // 16) * 16
    order = work_order(experts)
    most = max(len(steps) for action, steps in order if action == "U")
    hidden_width = expert_gate.shape[2]
    reach = -(-(toks + 2 * WINDOW) // 128) * 128
    padded = (tps - 1) * toks + reach
    vmem = pl.BlockSpec(memory_space=pltpu.VMEM)
    hbm = pl.BlockSpec(memory_space=pl.ANY)
    bf16 = jnp.bfloat16
    dma = pltpu.SemaphoreType.DMA
    small = (
        queries,
        keys,
        values,
        doc_ids[None, :],
        sink_logits[None, :],
        norm1_gain[None, :],
        norm1_bias[None, :],
        route_ids.T,
        route_weights.T,
        norm2_gain[None, :],
        norm2_bias[None, :],
        resid,
        out_proj,
    )
    return pl.pallas_call(
        functools.partial(layer_kernel, experts, tps, order),
        out_shape=jax.ShapeDtypeStruct((toks, width), bf16),
        in_specs=[hbm] * 16,
        out_specs=vmem,
        scratch_shapes=[pltpu.VMEM(a.shape, a.dtype) for a in small]
        + [
            pltpu.VMEM((padded, kv_width), bf16),
            pltpu.VMEM((padded, kv_width), bf16),
            pltpu.VMEM((2, 1, tok_dev), jnp.int32),
            pltpu.VMEM((tps, 1, reach), jnp.int32),
            pltpu.VMEM((tok_dev, 128), jnp.int32),
            pltpu.VMEM((toks, queries.shape[1]), bf16),
            pltpu.VMEM((tps, toks, width), bf16),
            pltpu.VMEM((tps, toks, width), bf16),
            pltpu.VMEM((toks, width), jnp.float32),
            pltpu.VMEM((toks, width), bf16),
            pltpu.VMEM((experts * capacity, toks), bf16),
            pltpu.VMEM((2, experts * capacity, toks), bf16),
            pltpu.VMEM((experts, capacity, width), bf16),
            pltpu.VMEM((experts, tps, capacity, width), bf16),
            pltpu.VMEM((width, hidden_width), bf16),
            pltpu.VMEM((width, hidden_width), bf16),
            pltpu.VMEM((hidden_width, width), bf16),
            pltpu.VMEM((most * tps * capacity, hidden_width), bf16),
            pltpu.VMEM((experts, tps, capacity, width), bf16),
            pltpu.VMEM((experts, tps, capacity, width), bf16),
            pltpu.VMEM((experts, capacity, width), bf16),
            pltpu.VMEM((experts, capacity, width), bf16),
            dma((16,)),
            dma((experts,)),
            dma((experts,)),
            dma((experts, tps)),
            dma((experts, tps)),
            dma((experts, tps)),
            dma((experts, tps)),
            dma((experts,)),
            dma((experts,)),
            dma((6,)),
            dma((6,)),
            dma((tps, width // HEAD_TILE)),
            dma((tps, width // HEAD_TILE)),
        ],
        compiler_params=pltpu.CompilerParams(
            collective_id=0, has_side_effects=True, vmem_limit_bytes=60 * 1024 * 1024
        ),
    )(*small, expert_gate, expert_up, expert_down)


def solution(mesh):
    return jax.shard_map(
        per_device,
        mesh=mesh,
        in_specs=(
            P(("grp", "sp", "tp"), None),
            P(("grp", "sp"), "tp"),
            P(("grp", "sp"), "tp"),
            P(("grp", "sp"), "tp"),
            P(("grp", "sp")),
            P("tp"),
            P("tp", None),
            P(),
            P(),
            P(("grp", "sp", "tp"), None),
            P(("grp", "sp", "tp"), None),
            P("sp", None, "tp"),
            P("sp", None, "tp"),
            P("sp", "tp", None),
            P(),
            P(),
        ),
        out_specs=P(("grp", "sp", "tp"), None),
        check_vma=False,
    )
```

```python
import functools

import jax
import jax.numpy as jnp
from jax import lax
from jax.experimental import pallas as pl
from jax.experimental.pallas import tpu as pltpu
from jax.sharding import PartitionSpec as P

HEAD_DIM = 64
WINDOW = 128
MESH = pl.DeviceIdType.MESH
CHUNKS = 4
HEAD_TILE = 512
VMEM_BYTES = 67043328


norm_epsilon = 1e-05
residual_scale = 1.4142135623730951
masked_score = -1e30


def layer_norm(values, gain_vec, bias_vec):
    mean_val = jnp.mean(values, -1, keepdims=True)
    centred = values - mean_val
    variance = jnp.mean(centred * centred, -1, keepdims=True)
    return centred * lax.rsqrt(variance + norm_epsilon) * gain_vec + bias_vec


def step_partner(step, sp_pos, count, back):
    chip, core = sp_pos // 2, sp_pos % 2
    half = count // 4
    side, place = chip // half, chip % half
    pair, flip = step // 2, step % 2
    if pair == 0:
        turn, cross = 0, False
    elif pair <= half:
        turn, cross = pair - 1, True
    else:
        turn, cross = pair - half, False
    target_side = 1 - side if cross else side
    move = half - turn if back else turn
    target = target_side * half + (place + move) % half
    return target * 2 + (core + flip) % 2


def chain_of_four(sp_pos):
    chip, core = sp_pos // 2, sp_pos % 2
    inner = chip * (3 - chip) // 2
    return chip, core, inner, chip + 1 - 2 * (chip % 2)


def target_of(step, sp_pos, count):
    if count != 8:
        return step_partner(step, sp_pos, count, False), step
    chip, core, inner, near = chain_of_four(sp_pos)
    pair, flip = step // 2, step % 2
    to = (chip, (chip + 2) % 4, 3 - chip, near)[pair]
    place = (0, 2 + 2 * inner, 6, 4 - 2 * inner)[pair]
    return to * 2 + (core + flip) % 2, place + flip


def source_of(slot, sp_pos, count):
    if count != 8:
        return step_partner(slot, sp_pos, count, True)
    chip, core, inner, near = chain_of_four(sp_pos)
    pair, flip = slot // 2, slot % 2
    even, far = (chip + 2) % 4, 3 - chip
    of = (
        chip,
        inner * even + (1 - inner) * near,
        inner * near + (1 - inner) * even,
        far,
    )[pair]
    return of * 2 + (core + flip) % 2


def dispatch_order(count):
    return (1, 2, 3, 6, 7, 4, 5) if count == 8 else range(1, count)


def work_order(count):
    if count == 8:
        return [
            ("F", (0,)),
            ("F", (1,)),
            ("F", (2,)),
            ("U", (0, 1,)),
            ("F", (3,)),
            ("D", (0, 1,)),
            ("X", (0,)),
            ("U", (2,)),
            ("D", (2,)),
            ("X", (2,)),
            ("F", (4,)),
            ("U", (3,)),
            ("D", (3,)),
            ("X", (3,)),
            ("F", (5,)),
            ("U", (4,)),
            ("F", (6,)),
            ("D", (4,)),
            ("X", (4,)),
            ("G", (2,)),
            ("U", (5,)),
            ("F", (7,)),
            ("D", (5,)),
            ("X", (5,)),
            ("G", (3,)),
            ("G", (4,)),
            ("U", (6,)),
            ("D", (6,)),
            ("X", (6,)),
            ("U", (7,)),
            ("D", (7,)),
            ("X", (7,)),
            ("G", (5,)),
            ("G", (6,)),
            ("X", (1,)),
            ("G", (7,)),
            ("G", (0,)),
            ("G", (1,)),
        ]
    chunk = count // CHUNKS
    groups = [tuple(range(c * chunk, (c + 1) * chunk)) for c in range(CHUNKS)]
    order = [("F", groups[0])]
    for c, group in enumerate(groups):
        order.append(("U", group))
        if c + 1 < CHUNKS:
            order.append(("F", groups[c + 1]))
        order += [("D", group), ("X", group)]
        if c > 0:
            order.append(("G", groups[c - 1]))
    return order + [("G", groups[-1])]


def head_copy(d, i, t, tps, head_part, head_peer, head_send, head_recv):
    cols = pl.ds(pl.multiple_of(i * HEAD_TILE, HEAD_TILE), HEAD_TILE)
    return pltpu.make_async_remote_copy(
        src_ref=head_part.at[d, :, cols],
        dst_ref=head_peer.at[d, :, cols],
        send_sem=head_send.at[d, i],
        recv_sem=head_recv.at[d, i],
        device_id={"tp": (t + d) % tps},
        device_id_type=MESH,
    )


def attend(
    count,
    tps,
    queries_ref,
    keys_ref,
    values_ref,
    docs_ref,
    sink_ref,
    proj_w,
    key_pad,
    value_pad,
    doc_side,
    doc_rows,
    doc_cols,
    attended,
    head_part,
    head_peer,
    halo_send,
    halo_recv,
    head_send,
    head_recv,
    barrier,
    kv_copies,
    query_copies,
    proj_copy,
):
    me, t = lax.axis_index("sp"), lax.axis_index("tp")
    tok_dev, tok_sub = queries_ref.shape[0], attended.shape[0]
    local_kv = keys_ref.shape[1] // HEAD_DIM
    heads = queries_ref.shape[1] // HEAD_DIM
    groups = heads // local_kv
    reach = doc_rows.shape[2]
    end = WINDOW + tok_dev
    rest = key_pad.shape[0] - end - WINDOW
    for copy in kv_copies:
        copy.wait()
    pl.semaphore_wait(barrier, count - 1 + tps - 1)
    copies = []
    for side in range(2):
        start, place = (tok_dev - WINDOW, 0) if side == 0 else (0, end)
        to = (me + 1) % count if side == 0 else (me + count - 1) % count
        pairs = (
            (keys_ref.at[pl.ds(start, WINDOW)], key_pad.at[pl.ds(place, WINDOW)]),
            (values_ref.at[pl.ds(start, WINDOW)], value_pad.at[pl.ds(place, WINDOW)]),
            (docs_ref, doc_side.at[side]),
        )
        for i, (own, pad) in enumerate(pairs):
            copies.append(
                pltpu.make_async_remote_copy(
                    src_ref=own,
                    dst_ref=pad,
                    send_sem=halo_send.at[2 * i + side],
                    recv_sem=halo_recv.at[2 * i + side],
                    device_id={"sp": to},
                    device_id_type=MESH,
                )
            )
    for copy in copies:
        copy.start()
    for pad, own in ((key_pad, keys_ref), (value_pad, values_ref)):
        pad[WINDOW:end] = own[...]
        if rest:
            pad[end + WINDOW :] = jnp.zeros((rest, pad.shape[1]), pad.dtype)
    doc_cols[...] = jnp.transpose(jnp.broadcast_to(docs_ref[...], (128, tok_dev)))
    for copy in query_copies:
        copy.wait()
    for copy in copies:
        copy.wait_recv()
    doc_row = jnp.concatenate(
        [doc_side[0][:, tok_dev - WINDOW :], docs_ref[...], doc_side[1][:, :WINDOW]]
        + ([jnp.zeros((1, rest), jnp.int32)] if rest else []),
        1,
    )
    for j in range(tps):
        doc_rows[j] = doc_row[:, j * tok_sub : j * tok_sub + reach]

    tile = HEAD_TILE
    width = proj_w.shape[1]
    for d in list(range(1, tps)) + [0]:
        block = (t + d) % tps
        base = pl.multiple_of(block * tok_sub, 16)
        key_block = key_pad[pl.ds(base, reach), :].astype(jnp.float32)
        value_block = value_pad[pl.ds(base, reach), :].astype(jnp.float32)
        key_docs = doc_rows[block]
        query_docs = doc_cols[pl.ds(base, tok_sub), 0:1]
        row = lax.broadcasted_iota(jnp.int32, (tok_sub, reach), 0)
        col = lax.broadcasted_iota(jnp.int32, (tok_sub, reach), 1)
        position = me * tok_dev + base - WINDOW + col
        allowed = (position >= 0) & (position < count * tok_dev)
        allowed = allowed & (col >= row) & (col <= row + 2 * WINDOW)
        allowed = allowed & (query_docs == key_docs)
        bias = jnp.where(allowed, 0.0, masked_score)
        low = lax.broadcasted_iota(jnp.int32, (1, 2 * HEAD_DIM), 1) < HEAD_DIM
        pairs = groups // 2
        for g in range(local_kv):
            span = slice(g // 2 * 2 * HEAD_DIM, g // 2 * 2 * HEAD_DIM + 2 * HEAD_DIM)
            key_side, value_side = key_block[:, span], value_block[:, span]
            if key_side.shape[1] < 2 * HEAD_DIM:
                blank = jnp.zeros((reach, HEAD_DIM), jnp.float32)
                key_side = jnp.concatenate([key_side, blank], 1)
                value_side = jnp.concatenate([value_side, blank], 1)
            here = low if g % 2 == 0 else jnp.logical_not(low)
            key_side = jnp.where(here, key_side, 0.0).astype(jnp.bfloat16)
            value_side = jnp.where(here, value_side, 1.0).astype(jnp.bfloat16)
            first = g * groups
            query = [
                queries_ref[
                    pl.ds(base, tok_sub),
                    (first + 2 * p) * HEAD_DIM : (first + 2 * p + 2) * HEAD_DIM,
                ].astype(jnp.float32)
                * HEAD_DIM ** (-0.5)
                for p in range(pairs)
            ]
            ratios = []
            for parity in range(2):
                turned = parity != g % 2
                stack = jnp.concatenate(
                    [pltpu.roll(q, HEAD_DIM, 1) if turned else q for q in query], 0
                ).astype(jnp.bfloat16)
                scores = lax.dot_general(
                    stack, key_side, (((1,), (1,)), ((), ())), preferred_element_type=jnp.float32
                )
                weights, sinks = [], []
                for p in range(pairs):
                    head = first + 2 * p + parity
                    sink = sink_ref[:, head : head + 1]
                    score = scores[p * tok_sub : (p + 1) * tok_sub] + bias
                    top = jnp.maximum(jnp.max(score, -1, keepdims=True), sink)
                    weights.append(jnp.exp(score - top).astype(jnp.bfloat16))
                    sinks.append(jnp.exp(sink - top))
                result = jnp.dot(
                    jnp.concatenate(weights, 0), value_side, preferred_element_type=jnp.float32
                )
                other = pltpu.roll(result, HEAD_DIM, 1)
                top_side, sum_side = (other, result) if turned else (result, other)
                ratios.append(top_side / (sum_side + jnp.concatenate(sinks, 0)))
            joined = jnp.where(low, ratios[0], ratios[1]).astype(jnp.bfloat16)
            for p in range(pairs):
                lane = (first + 2 * p) * HEAD_DIM
                attended[:, lane : lane + 2 * HEAD_DIM] = joined[p * tok_sub : (p + 1) * tok_sub]
        if d == 1 or tps == 1:
            proj_copy.wait()

        def project(i, carry):
            cols = pl.ds(pl.multiple_of(i * tile, tile), tile)
            head_part[d, :, cols] = jnp.dot(
                attended[...], proj_w[:, cols], preferred_element_type=jnp.float32
            ).astype(jnp.bfloat16)
            if d:
                head_copy(d, i, t, tps, head_part, head_peer, head_send, head_recv).start()
            return carry

        lax.fori_loop(0, width // tile, project, 0)
    for copy in copies:
        copy.wait_send()


def layer_kernel(
    experts,
    tps,
    order,
    queries_hbm,
    keys_hbm,
    values_hbm,
    docs_hbm,
    sink_hbm,
    gain1_hbm,
    bias1_hbm,
    ids_hbm,
    mix_hbm,
    gain_hbm,
    bias_hbm,
    resid_hbm,
    proj_hbm,
    gate_hbm,
    up_hbm,
    down_hbm,
    out_ref,
    queries_ref,
    keys_ref,
    values_ref,
    docs_ref,
    sink_ref,
    gain1_ref,
    bias1_ref,
    ids_ref,
    mix_ref,
    gain_ref,
    bias_ref,
    resid_ref,
    proj_w,
    key_pad,
    value_pad,
    doc_side,
    doc_rows,
    doc_cols,
    attended,
    head_part,
    head_peer,
    pre_ref,
    normed_ref,
    assign_ref,
    combine_ref,
    outgoing,
    rows,
    gate_w,
    up_w,
    down_w,
    hidden,
    part,
    peer,
    summed,
    returned,
    in_sem,
    disp_send,
    disp_recv,
    fwd_send,
    fwd_recv,
    part_send,
    part_recv,
    ret_send,
    ret_recv,
    halo_send,
    halo_recv,
    head_send,
    head_recv,
):
    me, t = lax.axis_index("sp"), lax.axis_index("tp")
    _, capacity, width = outgoing.shape
    toks = normed_ref.shape[0]

    barrier = pltpu.get_barrier_semaphore()
    for d in range(1, experts):
        pl.semaphore_signal(
            barrier, inc=1, device_id={"sp": (me + d) % experts}, device_id_type=MESH
        )
    for d in range(1, tps):
        pl.semaphore_signal(barrier, inc=1, device_id={"tp": (t + d) % tps}, device_id_type=MESH)

    places = (
        (keys_hbm, keys_ref),
        (values_hbm, values_ref),
        (docs_hbm, docs_ref),
        (queries_hbm, queries_ref),
        (sink_hbm, sink_ref),
        (proj_hbm, proj_w),
        (ids_hbm, ids_ref),
        (mix_hbm, mix_ref),
        (resid_hbm, resid_ref),
        (gain1_hbm, gain1_ref),
        (bias1_hbm, bias1_ref),
        (gain_hbm, gain_ref),
        (bias_hbm, bias_ref),
        (gate_hbm.at[0], gate_w),
        (up_hbm.at[0], up_w),
        (down_hbm.at[0], down_w),
    )
    loads = [
        pltpu.make_async_copy(source, place, in_sem.at[i])
        for i, (source, place) in enumerate(places)
    ]
    for load in loads:
        load.start()
    weight_loads = loads[13:]

    attend(
        experts,
        tps,
        queries_ref,
        keys_ref,
        values_ref,
        docs_ref,
        sink_ref,
        proj_w,
        key_pad,
        value_pad,
        doc_side,
        doc_rows,
        doc_cols,
        attended,
        head_part,
        head_peer,
        halo_send,
        halo_recv,
        head_send,
        head_recv,
        barrier,
        loads[:3],
        loads[3:5],
        loads[5],
    )
    for load in loads[6:13]:
        load.wait()
    lanes = experts * capacity
    top = ids_ref.shape[0]
    expert_iota = lax.broadcasted_iota(jnp.int32, (experts, toks), 0)
    upper = (
        lax.broadcasted_iota(jnp.int32, (toks, toks), 0)
        < lax.broadcasted_iota(jnp.int32, (toks, toks), 1)
    ).astype(jnp.float32).astype(jnp.bfloat16)
    before = jnp.zeros((experts, 1), jnp.float32)
    slot_iota = lax.broadcasted_iota(jnp.int32, (lanes, toks), 0)
    assign = jnp.zeros((lanes, toks), jnp.float32)
    combine = jnp.zeros((lanes, toks), jnp.float32)
    for k in range(top):
        own = ids_ref[k : k + 1, :]
        hot = (own == expert_iota).astype(jnp.float32)
        rank = before + jnp.dot(hot.astype(jnp.bfloat16), upper, preferred_element_type=jnp.float32)
        rank = jnp.sum(rank * hot, axis=0, keepdims=True).astype(jnp.int32)
        before = before + jnp.sum(hot, axis=1, keepdims=True)
        match = (own * capacity + rank == slot_iota).astype(jnp.float32)
        assign = assign + match
        combine = combine + match * mix_ref[k : k + 1, :]
    assign_ref[...] = assign.astype(jnp.bfloat16)
    high = combine.astype(jnp.bfloat16)
    combine_ref[0] = high
    combine_ref[1] = (combine - high.astype(jnp.float32)).astype(jnp.bfloat16)

    total = jnp.zeros((toks, 1), jnp.float32)
    for i in range(width // HEAD_TILE):
        cols = slice(i * HEAD_TILE, (i + 1) * HEAD_TILE)
        projected = head_part[0, :, cols].astype(jnp.float32)
        for d in range(1, tps):
            head_copy(d, i, t, tps, head_part, head_peer, head_send, head_recv).wait_recv()
            projected = projected + head_peer[d, :, cols].astype(jnp.float32)
        projected = projected.astype(jnp.bfloat16).astype(jnp.float32)
        pre_norm = residual_scale * resid_ref[:, cols].astype(jnp.float32) + projected
        pre_ref[:, cols] = pre_norm
        total = total + jnp.sum(pre_norm, -1, keepdims=True)
    centred = pre_ref[...] - total * (1.0 / width)
    variance = jnp.mean(centred * centred, -1, keepdims=True)
    normed = centred * lax.rsqrt(variance + norm_epsilon) * gain1_ref[...] + bias1_ref[...]
    normed_ref[...] = normed.astype(jnp.bfloat16)
    spread = jnp.dot(assign_ref[...], normed_ref[...], preferred_element_type=jnp.float32)
    outgoing[...] = spread.astype(jnp.bfloat16).reshape(experts, capacity, width)

    def dispatch(step):
        dst, slot = target_of(step, me, experts)
        return pltpu.make_async_remote_copy(
            src_ref=outgoing.at[dst],
            dst_ref=rows.at[slot, t],
            send_sem=disp_send.at[step],
            recv_sem=disp_recv.at[slot],
            device_id={"sp": dst},
            device_id_type=MESH,
        )

    def arrived(slot):
        return pltpu.make_async_remote_copy(
            src_ref=outgoing.at[slot],
            dst_ref=rows.at[slot, t],
            send_sem=disp_send.at[slot],
            recv_sem=disp_recv.at[slot],
            device_id={"sp": source_of(slot, me, experts)},
            device_id_type=MESH,
        )

    def forward(step, d):
        dst = (t + d) % tps
        return pltpu.make_async_remote_copy(
            src_ref=rows.at[step, t],
            dst_ref=rows.at[step, t],
            send_sem=fwd_send.at[step, d],
            recv_sem=fwd_recv.at[step, d],
            device_id={"tp": dst},
            device_id_type=MESH,
        )

    def share(step, d):
        dst = (t + d) % tps
        return pltpu.make_async_remote_copy(
            src_ref=part.at[step, dst],
            dst_ref=peer.at[step, d],
            send_sem=part_send.at[step, d],
            recv_sem=part_recv.at[step, d],
            device_id={"tp": dst},
            device_id_type=MESH,
        )

    def give_back(step):
        return pltpu.make_async_remote_copy(
            src_ref=summed.at[step],
            dst_ref=returned.at[me],
            send_sem=ret_send.at[step],
            recv_sem=ret_recv.at[me],
            device_id={"sp": source_of(step, me, experts)},
            device_id_type=MESH,
        )

    for step in dispatch_order(experts):
        dispatch(step).start()
    rows[0, t] = outgoing[me]

    def send_on(step):
        if step > 0:
            arrived(step).wait_recv()
        for d in range(1, tps):
            forward(step, d).start()

    def finish(step):
        total = part[step, t].astype(jnp.float32)
        for d in range(1, tps):
            share(step, d).wait_recv()
            total = total + peer[step, d].astype(jnp.float32)
        if step == 0:
            returned[me] = total.astype(jnp.bfloat16)
        else:
            summed[step] = total.astype(jnp.bfloat16)
            give_back(step).start()

    tile = 512 if gate_w.shape[1] % 512 == 0 else 256
    hidden_width = gate_w.shape[1]

    def up_stage(k0, k1):
        m = (k1 - k0) * tps * capacity
        for step in range(k0, k1):
            for d in range(1, tps):
                forward(step, d).wait_recv()

        def up_tile(i, carry):
            cols = pl.ds(pl.multiple_of(i * tile, tile), tile)
            block = rows[k0:k1].reshape(m, width)
            gate = jnp.dot(block, gate_w[:, cols], preferred_element_type=jnp.float32)
            up = jnp.dot(block, up_w[:, cols], preferred_element_type=jnp.float32)
            hidden[:m, cols] = (gate / (1.0 + jnp.exp(-gate)) * up).astype(jnp.bfloat16)
            return carry

        lax.fori_loop(0, hidden_width // tile, up_tile, 0)

    def down_stage(k0, k1):
        m = (k1 - k0) * tps * capacity

        def down_tile(i, carry):
            cols = pl.ds(pl.multiple_of(i * tile, tile), tile)
            result = jnp.dot(hidden[:m], down_w[:, cols], preferred_element_type=jnp.float32)
            part[k0:k1, :, :, cols] = result.astype(jnp.bfloat16).reshape(
                k1 - k0, tps, capacity, tile
            )
            return carry

        lax.fori_loop(0, width // tile, down_tile, 0)

    waiting = {"U": weight_loads[:2], "D": weight_loads[2:]}
    for action, steps in order:
        for load in waiting.pop(action, ()):
            load.wait()
        with jax.named_scope(f"{action}{steps[0]}"):
            if action == "U":
                up_stage(steps[0], steps[-1] + 1)
            elif action == "D":
                down_stage(steps[0], steps[-1] + 1)
            else:
                for step in steps:
                    if action == "F":
                        send_on(step)
                    elif action == "G":
                        finish(step)
                    else:
                        for d in range(1, tps):
                            share(step, d).start()

    for d in range(1, experts):
        src = (me + d) % experts
        pltpu.make_async_remote_copy(
            src_ref=summed.at[d],
            dst_ref=returned.at[src],
            send_sem=ret_send.at[d],
            recv_sem=ret_recv.at[src],
            device_id={"sp": src},
            device_id_type=MESH,
        ).wait_recv()

    back = returned[...].reshape(lanes, width)
    across = (((0,), (0,)), ((), ()))
    moe_sum = lax.dot_general(combine_ref[0], back, across, preferred_element_type=jnp.float32)
    moe_sum = moe_sum + lax.dot_general(
        combine_ref[1], back, across, preferred_element_type=jnp.float32
    )
    pre_final = residual_scale * normed_ref[...].astype(jnp.float32) + moe_sum
    out_ref[...] = layer_norm(pre_final, gain_ref[...], bias_ref[...]).astype(jnp.bfloat16)

    for d in range(1, tps):
        for i in range(width // HEAD_TILE):
            head_copy(d, i, t, tps, head_part, head_peer, head_send, head_recv).wait_send()
    for step in range(experts):
        if step > 0:
            dispatch(step).wait_send()
            give_back(step).wait_send()
        for d in range(1, tps):
            forward(step, d).wait_send()
            share(step, d).wait_send()


def per_device(
    resid,
    queries,
    keys,
    values,
    doc_ids,
    sink_logits,
    out_proj,
    norm1_gain,
    norm1_bias,
    route_ids,
    route_weights,
    expert_gate,
    expert_up,
    expert_down,
    norm2_gain,
    norm2_bias,
):
    experts, tps = lax.axis_size("sp"), lax.axis_size("tp")
    toks, width = resid.shape
    tok_dev, kv_width = keys.shape
    need = 5 * toks // (2 * experts)
    capacity = -(-need // 16) * 16
    order = work_order(experts)
    most = max(len(steps) for action, steps in order if action == "U")
    hidden_width = expert_gate.shape[2]
    reach = -(-(toks + 2 * WINDOW) // 128) * 128
    padded = (tps - 1) * toks + reach
    vmem = pl.BlockSpec(memory_space=pltpu.VMEM)
    hbm = pl.BlockSpec(memory_space=pltpu.HBM)
    bf16 = jnp.bfloat16
    dma = pltpu.SemaphoreType.DMA
    small = (
        queries,
        keys,
        values,
        doc_ids[None, :],
        sink_logits[None, :],
        norm1_gain[None, :],
        norm1_bias[None, :],
        route_ids.T,
        route_weights.T,
        norm2_gain[None, :],
        norm2_bias[None, :],
        resid,
        out_proj,
    )
    return pl.pallas_call(
        functools.partial(layer_kernel, experts, tps, order),
        out_shape=pltpu.VMEM((toks, width), bf16),
        in_specs=[hbm] * 16,
        out_specs=vmem,
        scratch_shapes=[pltpu.VMEM(a.shape, a.dtype) for a in small]
        + [
            pltpu.VMEM((padded, kv_width), bf16),
            pltpu.VMEM((padded, kv_width), bf16),
            pltpu.VMEM((2, 1, tok_dev), jnp.int32),
            pltpu.VMEM((tps, 1, reach), jnp.int32),
            pltpu.VMEM((tok_dev, 128), jnp.int32),
            pltpu.VMEM((toks, queries.shape[1]), bf16),
            pltpu.VMEM((tps, toks, width), bf16),
            pltpu.VMEM((tps, toks, width), bf16),
            pltpu.VMEM((toks, width), jnp.float32),
            pltpu.VMEM((toks, width), bf16),
            pltpu.VMEM((experts * capacity, toks), bf16),
            pltpu.VMEM((2, experts * capacity, toks), bf16),
            pltpu.VMEM((experts, capacity, width), bf16),
            pltpu.VMEM((experts, tps, capacity, width), bf16),
            pltpu.VMEM((width, hidden_width), bf16),
            pltpu.VMEM((width, hidden_width), bf16),
            pltpu.VMEM((hidden_width, width), bf16),
            pltpu.VMEM((most * tps * capacity, hidden_width), bf16),
            pltpu.VMEM((experts, tps, capacity, width), bf16),
            pltpu.VMEM((experts, tps, capacity, width), bf16),
            pltpu.VMEM((experts, capacity, width), bf16),
            pltpu.VMEM((experts, capacity, width), bf16),
            dma((16,)),
            dma((experts,)),
            dma((experts,)),
            dma((experts, tps)),
            dma((experts, tps)),
            dma((experts, tps)),
            dma((experts, tps)),
            dma((experts,)),
            dma((experts,)),
            dma((6,)),
            dma((6,)),
            dma((tps, width // HEAD_TILE)),
            dma((tps, width // HEAD_TILE)),
        ],
        compiler_params=pltpu.CompilerParams(
            collective_id=0, has_side_effects=True, vmem_limit_bytes=VMEM_BYTES - 2 * toks * width
        ),
    )(*small, expert_gate, expert_up, expert_down)


def solution(mesh):
    return jax.shard_map(
        per_device,
        mesh=mesh,
        in_specs=(
            P(("grp", "sp", "tp"), None),
            P(("grp", "sp"), "tp"),
            P(("grp", "sp"), "tp"),
            P(("grp", "sp"), "tp"),
            P(("grp", "sp")),
            P("tp"),
            P("tp", None),
            P(),
            P(),
            P(("grp", "sp", "tp"), None),
            P(("grp", "sp", "tp"), None),
            P("sp", None, "tp"),
            P("sp", None, "tp"),
            P("sp", "tp", None),
            P(),
            P(),
        ),
        out_specs=P(("grp", "sp", "tp"), None),
        check_vma=False,
    )
```

```python
import functools

import jax
import jax.numpy as jnp
from jax import lax
from jax.experimental import pallas as pl
from jax.experimental.pallas import tpu as pltpu
from jax.sharding import PartitionSpec as P

HEAD_DIM = 64
WINDOW = 128
MESH = pl.DeviceIdType.MESH
CHUNKS = 4
HEAD_TILE = 512
VMEM_BYTES = 67043328


norm_epsilon = 1e-05
residual_scale = 1.4142135623730951
masked_score = -1e30


def layer_norm(values, gain_vec, bias_vec):
    mean_val = jnp.mean(values, -1, keepdims=True)
    centred = values - mean_val
    variance = jnp.mean(centred * centred, -1, keepdims=True)
    return centred * lax.rsqrt(variance + norm_epsilon) * gain_vec + bias_vec


def step_partner(step, sp_pos, count, back):
    chip, core = sp_pos // 2, sp_pos % 2
    half = count // 4
    side, place = chip // half, chip % half
    pair, flip = step // 2, step % 2
    if pair == 0:
        turn, cross = 0, False
    elif pair <= half:
        turn, cross = pair - 1, True
    else:
        turn, cross = pair - half, False
    target_side = 1 - side if cross else side
    move = half - turn if back else turn
    target = target_side * half + (place + move) % half
    return target * 2 + (core + flip) % 2


def chain_of_four(sp_pos):
    chip, core = sp_pos // 2, sp_pos % 2
    inner = chip * (3 - chip) // 2
    return chip, core, inner, chip + 1 - 2 * (chip % 2)


def target_of(step, sp_pos, count):
    if count != 8:
        return step_partner(step, sp_pos, count, False), step
    chip, core, inner, near = chain_of_four(sp_pos)
    pair, flip = step // 2, step % 2
    to = (chip, (chip + 2) % 4, 3 - chip, near)[pair]
    place = (0, 2 + 2 * inner, 6, 4 - 2 * inner)[pair]
    return to * 2 + (core + flip) % 2, place + flip


def source_of(slot, sp_pos, count):
    if count != 8:
        return step_partner(slot, sp_pos, count, True)
    chip, core, inner, near = chain_of_four(sp_pos)
    pair, flip = slot // 2, slot % 2
    even, far = (chip + 2) % 4, 3 - chip
    of = (
        chip,
        inner * even + (1 - inner) * near,
        inner * near + (1 - inner) * even,
        far,
    )[pair]
    return of * 2 + (core + flip) % 2


def dispatch_order(count):
    return (1, 2, 3, 6, 7, 4, 5) if count == 8 else range(1, count)


def work_order(count):
    if count == 8:
        return [
            ("F", (0,)),
            ("F", (1,)),
            ("F", (2,)),
            ("U", (0, 1,)),
            ("F", (3,)),
            ("D", (0, 1,)),
            ("U", (2,)),
            ("F", (4,)),
            ("D", (2,)),
            ("X", (2,)),
            ("U", (3,)),
            ("F", (5,)),
            ("D", (3,)),
            ("X", (3,)),
            ("U", (4,)),
            ("F", (6,)),
            ("D", (4,)),
            ("G", (2,)),
            ("X", (4,)),
            ("U", (5,)),
            ("F", (7,)),
            ("D", (5,)),
            ("G", (3,)),
            ("X", (5,)),
            ("U", (6,)),
            ("G", (4,)),
            ("D", (6,)),
            ("X", (6,)),
            ("U", (7,)),
            ("G", (5,)),
            ("D", (7,)),
            ("X", (7,)),
            ("X", (0,)),
            ("X", (1,)),
            ("G", (6,)),
            ("G", (7,)),
            ("G", (0,)),
            ("G", (1,)),
        ]
    chunk = count // CHUNKS
    groups = [tuple(range(c * chunk, (c + 1) * chunk)) for c in range(CHUNKS)]
    order = [("F", groups[0])]
    for c, group in enumerate(groups):
        order.append(("U", group))
        if c + 1 < CHUNKS:
            order.append(("F", groups[c + 1]))
        order += [("D", group), ("X", group)]
        if c > 0:
            order.append(("G", groups[c - 1]))
    return order + [("G", groups[-1])]


def split_rows(toks, experts):
    need = 5 * toks // (2 * experts)
    whole, pairs = need // 8 * 8, -(-(need % 8) // 2)
    if whole == 0 or pairs in (0, 4):
        whole, pairs = -(-need // 16) * 16, 0
    return -(-need // 16) * 16, whole, pairs


class Copies:
    def __init__(self, source, target, send, recv, device, whole, pairs):
        ends = [(source[0].at[pl.ds(0, whole)], target[0].at[pl.ds(0, whole)])]
        if pairs:
            ends.append((source[1], target[1]))
        self.copies = [
            pltpu.make_async_remote_copy(
                src_ref=src,
                dst_ref=dst,
                send_sem=send.at[i],
                recv_sem=recv.at[i],
                device_id=device,
                device_id_type=MESH,
            )
            for i, (src, dst) in enumerate(ends)
        ]

    def start(self):
        for copy in self.copies:
            copy.start()

    def wait_recv(self):
        for copy in self.copies:
            copy.wait_recv()

    def wait_send(self):
        for copy in self.copies:
            copy.wait_send()


def head_copy(d, i, t, tps, head_part, head_peer, head_send, head_recv):
    cols = pl.ds(pl.multiple_of(i * HEAD_TILE, HEAD_TILE), HEAD_TILE)
    return pltpu.make_async_remote_copy(
        src_ref=head_part.at[d, :, cols],
        dst_ref=head_peer.at[d, :, cols],
        send_sem=head_send.at[d, i],
        recv_sem=head_recv.at[d, i],
        device_id={"tp": (t + d) % tps},
        device_id_type=MESH,
    )


def attend(
    count,
    tps,
    queries_ref,
    keys_ref,
    values_ref,
    docs_ref,
    sink_ref,
    proj_w,
    key_pad,
    value_pad,
    doc_side,
    doc_rows,
    doc_cols,
    attended,
    head_part,
    head_peer,
    halo_send,
    halo_recv,
    head_send,
    head_recv,
    barrier,
    kv_copies,
    query_copies,
    proj_copy,
):
    me, t = lax.axis_index("sp"), lax.axis_index("tp")
    tok_dev, tok_sub = queries_ref.shape[0], attended.shape[0]
    local_kv = keys_ref.shape[1] // HEAD_DIM
    heads = queries_ref.shape[1] // HEAD_DIM
    groups = heads // local_kv
    reach = doc_rows.shape[2]
    end = WINDOW + tok_dev
    rest = key_pad.shape[0] - end - WINDOW
    for copy in kv_copies:
        copy.wait()
    pl.semaphore_wait(barrier, count - 1 + tps - 1)
    copies = []
    for side in range(2):
        start, place = (tok_dev - WINDOW, 0) if side == 0 else (0, end)
        to = (me + 1) % count if side == 0 else (me + count - 1) % count
        pairs = (
            (keys_ref.at[pl.ds(start, WINDOW)], key_pad.at[pl.ds(place, WINDOW)]),
            (values_ref.at[pl.ds(start, WINDOW)], value_pad.at[pl.ds(place, WINDOW)]),
            (docs_ref, doc_side.at[side]),
        )
        for i, (own, pad) in enumerate(pairs):
            copies.append(
                pltpu.make_async_remote_copy(
                    src_ref=own,
                    dst_ref=pad,
                    send_sem=halo_send.at[2 * i + side],
                    recv_sem=halo_recv.at[2 * i + side],
                    device_id={"sp": to},
                    device_id_type=MESH,
                )
            )
    for copy in copies:
        copy.start()
    for pad, own in ((key_pad, keys_ref), (value_pad, values_ref)):
        pad[WINDOW:end] = own[...]
        if rest:
            pad[end + WINDOW :] = jnp.zeros((rest, pad.shape[1]), pad.dtype)
    doc_cols[...] = jnp.transpose(jnp.broadcast_to(docs_ref[...], (128, tok_dev)))
    for copy in query_copies:
        copy.wait()
    for copy in copies:
        copy.wait_recv()
    doc_row = jnp.concatenate(
        [doc_side[0][:, tok_dev - WINDOW :], docs_ref[...], doc_side[1][:, :WINDOW]]
        + ([jnp.zeros((1, rest), jnp.int32)] if rest else []),
        1,
    )
    for j in range(tps):
        doc_rows[j] = doc_row[:, j * tok_sub : j * tok_sub + reach]

    tile = HEAD_TILE
    width = proj_w.shape[1]
    for d in list(range(1, tps)) + [0]:
        block = (t + d) % tps
        base = pl.multiple_of(block * tok_sub, 16)
        key_block = key_pad[pl.ds(base, reach), :].astype(jnp.float32)
        value_block = value_pad[pl.ds(base, reach), :].astype(jnp.float32)
        key_docs = doc_rows[block]
        query_docs = doc_cols[pl.ds(base, tok_sub), 0:1]
        row = lax.broadcasted_iota(jnp.int32, (tok_sub, reach), 0)
        col = lax.broadcasted_iota(jnp.int32, (tok_sub, reach), 1)
        position = me * tok_dev + base - WINDOW + col
        allowed = (position >= 0) & (position < count * tok_dev)
        allowed = allowed & (col >= row) & (col <= row + 2 * WINDOW)
        allowed = allowed & (query_docs == key_docs)
        bias = jnp.where(allowed, 0.0, masked_score)
        low = lax.broadcasted_iota(jnp.int32, (1, 2 * HEAD_DIM), 1) < HEAD_DIM
        pairs = groups // 2
        for g in range(local_kv):
            span = slice(g // 2 * 2 * HEAD_DIM, g // 2 * 2 * HEAD_DIM + 2 * HEAD_DIM)
            key_side, value_side = key_block[:, span], value_block[:, span]
            if key_side.shape[1] < 2 * HEAD_DIM:
                blank = jnp.zeros((reach, HEAD_DIM), jnp.float32)
                key_side = jnp.concatenate([key_side, blank], 1)
                value_side = jnp.concatenate([value_side, blank], 1)
            here = low if g % 2 == 0 else jnp.logical_not(low)
            key_side = jnp.where(here, key_side, 0.0).astype(jnp.bfloat16)
            value_side = jnp.where(here, value_side, 1.0).astype(jnp.bfloat16)
            first = g * groups
            query = [
                queries_ref[
                    pl.ds(base, tok_sub),
                    (first + 2 * p) * HEAD_DIM : (first + 2 * p + 2) * HEAD_DIM,
                ].astype(jnp.float32)
                * HEAD_DIM ** (-0.5)
                for p in range(pairs)
            ]
            ratios = []
            for parity in range(2):
                turned = parity != g % 2
                stack = jnp.concatenate(
                    [pltpu.roll(q, HEAD_DIM, 1) if turned else q for q in query], 0
                ).astype(jnp.bfloat16)
                scores = lax.dot_general(
                    stack, key_side, (((1,), (1,)), ((), ())), preferred_element_type=jnp.float32
                )
                weights, sinks = [], []
                for p in range(pairs):
                    head = first + 2 * p + parity
                    sink = sink_ref[:, head : head + 1]
                    score = scores[p * tok_sub : (p + 1) * tok_sub] + bias
                    top = jnp.maximum(jnp.max(score, -1, keepdims=True), sink)
                    weights.append(jnp.exp(score - top).astype(jnp.bfloat16))
                    sinks.append(jnp.exp(sink - top))
                result = jnp.dot(
                    jnp.concatenate(weights, 0), value_side, preferred_element_type=jnp.float32
                )
                other = pltpu.roll(result, HEAD_DIM, 1)
                top_side, sum_side = (other, result) if turned else (result, other)
                ratios.append(top_side / (sum_side + jnp.concatenate(sinks, 0)))
            joined = jnp.where(low, ratios[0], ratios[1]).astype(jnp.bfloat16)
            for p in range(pairs):
                lane = (first + 2 * p) * HEAD_DIM
                attended[:, lane : lane + 2 * HEAD_DIM] = joined[p * tok_sub : (p + 1) * tok_sub]
        if d == 1 or tps == 1:
            proj_copy.wait()

        def project(i, carry):
            cols = pl.ds(pl.multiple_of(i * tile, tile), tile)
            head_part[d, :, cols] = jnp.dot(
                attended[...], proj_w[:, cols], preferred_element_type=jnp.float32
            ).astype(jnp.bfloat16)
            if d:
                head_copy(d, i, t, tps, head_part, head_peer, head_send, head_recv).start()
            return carry

        lax.fori_loop(0, width // tile, project, 0)
    for copy in copies:
        copy.wait_send()


def layer_kernel(
    experts,
    tps,
    order,
    queries_hbm,
    keys_hbm,
    values_hbm,
    docs_hbm,
    sink_hbm,
    gain1_hbm,
    bias1_hbm,
    ids_hbm,
    mix_hbm,
    gain_hbm,
    bias_hbm,
    resid_hbm,
    proj_hbm,
    gate_hbm,
    up_hbm,
    down_hbm,
    out_ref,
    queries_ref,
    keys_ref,
    values_ref,
    docs_ref,
    sink_ref,
    gain1_ref,
    bias1_ref,
    ids_ref,
    mix_ref,
    gain_ref,
    bias_ref,
    resid_ref,
    proj_w,
    key_pad,
    value_pad,
    doc_side,
    doc_rows,
    doc_cols,
    attended,
    head_part,
    head_peer,
    pre_ref,
    normed_ref,
    assign_ref,
    combine_ref,
    outgoing,
    outgoing_pairs,
    rows,
    rows_pairs,
    gate_w,
    up_w,
    down_w,
    hidden,
    part,
    part_pairs,
    peer,
    peer_pairs,
    summed,
    summed_pairs,
    returned,
    returned_pairs,
    in_sem,
    disp_send,
    disp_recv,
    fwd_send,
    fwd_recv,
    part_send,
    part_recv,
    ret_send,
    ret_recv,
    halo_send,
    halo_recv,
    head_send,
    head_recv,
):
    me, t = lax.axis_index("sp"), lax.axis_index("tp")
    width = outgoing.shape[2]
    toks = normed_ref.shape[0]
    capacity, whole, pairs = split_rows(toks, experts)

    def take_pairs(block, block_pairs):
        for i in range(pairs):
            block[whole + 2 * i : whole + 2 * i + 2] = block_pairs[i]


    barrier = pltpu.get_barrier_semaphore()
    for d in range(1, experts):
        pl.semaphore_signal(
            barrier, inc=1, device_id={"sp": (me + d) % experts}, device_id_type=MESH
        )
    for d in range(1, tps):
        pl.semaphore_signal(barrier, inc=1, device_id={"tp": (t + d) % tps}, device_id_type=MESH)

    places = (
        (keys_hbm, keys_ref),
        (values_hbm, values_ref),
        (docs_hbm, docs_ref),
        (queries_hbm, queries_ref),
        (sink_hbm, sink_ref),
        (proj_hbm, proj_w),
        (ids_hbm, ids_ref),
        (mix_hbm, mix_ref),
        (resid_hbm, resid_ref),
        (gain1_hbm, gain1_ref),
        (bias1_hbm, bias1_ref),
        (gain_hbm, gain_ref),
        (bias_hbm, bias_ref),
        (gate_hbm.at[0], gate_w),
        (up_hbm.at[0], up_w),
        (down_hbm.at[0], down_w),
    )
    loads = [
        pltpu.make_async_copy(source, place, in_sem.at[i])
        for i, (source, place) in enumerate(places)
    ]
    for load in loads:
        load.start()
    weight_loads = loads[13:]

    attend(
        experts,
        tps,
        queries_ref,
        keys_ref,
        values_ref,
        docs_ref,
        sink_ref,
        proj_w,
        key_pad,
        value_pad,
        doc_side,
        doc_rows,
        doc_cols,
        attended,
        head_part,
        head_peer,
        halo_send,
        halo_recv,
        head_send,
        head_recv,
        barrier,
        loads[:3],
        loads[3:5],
        loads[5],
    )
    for load in loads[6:13]:
        load.wait()
    lanes = experts * capacity
    top = ids_ref.shape[0]
    expert_iota = lax.broadcasted_iota(jnp.int32, (experts, toks), 0)
    upper = (
        lax.broadcasted_iota(jnp.int32, (toks, toks), 0)
        < lax.broadcasted_iota(jnp.int32, (toks, toks), 1)
    ).astype(jnp.float32).astype(jnp.bfloat16)
    before = jnp.zeros((experts, 1), jnp.float32)
    slot_iota = lax.broadcasted_iota(jnp.int32, (lanes, toks), 0)
    assign = jnp.zeros((lanes, toks), jnp.float32)
    combine = jnp.zeros((lanes, toks), jnp.float32)
    for k in range(top):
        own = ids_ref[k : k + 1, :]
        hot = (own == expert_iota).astype(jnp.float32)
        rank = before + jnp.dot(hot.astype(jnp.bfloat16), upper, preferred_element_type=jnp.float32)
        rank = jnp.sum(rank * hot, axis=0, keepdims=True).astype(jnp.int32)
        before = before + jnp.sum(hot, axis=1, keepdims=True)
        match = (own * capacity + rank == slot_iota).astype(jnp.float32)
        assign = assign + match
        combine = combine + match * mix_ref[k : k + 1, :]
    assign_ref[...] = assign.astype(jnp.bfloat16)
    high = combine.astype(jnp.bfloat16)
    combine_ref[0] = high
    combine_ref[1] = (combine - high.astype(jnp.float32)).astype(jnp.bfloat16)

    total = jnp.zeros((toks, 1), jnp.float32)
    for i in range(width // HEAD_TILE):
        cols = slice(i * HEAD_TILE, (i + 1) * HEAD_TILE)
        projected = head_part[0, :, cols].astype(jnp.float32)
        for d in range(1, tps):
            head_copy(d, i, t, tps, head_part, head_peer, head_send, head_recv).wait_recv()
            projected = projected + head_peer[d, :, cols].astype(jnp.float32)
        projected = projected.astype(jnp.bfloat16).astype(jnp.float32)
        pre_norm = residual_scale * resid_ref[:, cols].astype(jnp.float32) + projected
        pre_ref[:, cols] = pre_norm
        total = total + jnp.sum(pre_norm, -1, keepdims=True)
    centred = pre_ref[...] - total * (1.0 / width)
    variance = jnp.mean(centred * centred, -1, keepdims=True)
    normed = centred * lax.rsqrt(variance + norm_epsilon) * gain1_ref[...] + bias1_ref[...]
    normed_ref[...] = normed.astype(jnp.bfloat16)
    spread = jnp.dot(assign_ref[...], normed_ref[...], preferred_element_type=jnp.float32)
    outgoing[...] = spread.astype(jnp.bfloat16).reshape(experts, capacity, width)
    for e in range(experts):
        for i in range(pairs):
            row = whole + 2 * i
            outgoing_pairs[e, i] = outgoing[e, row : row + 2]

    def move(source, target, send, recv, device):
        return Copies(source, target, send, recv, device, whole, pairs)

    def dispatch(step):
        dst, slot = target_of(step, me, experts)
        return move(
            (outgoing.at[dst], outgoing_pairs.at[dst]),
            (rows.at[slot, t], rows_pairs.at[slot, t]),
            disp_send.at[step],
            disp_recv.at[slot],
            {"sp": dst},
        )

    def arrived(slot):
        return move(
            (outgoing.at[slot], outgoing_pairs.at[slot]),
            (rows.at[slot, t], rows_pairs.at[slot, t]),
            disp_send.at[slot],
            disp_recv.at[slot],
            {"sp": source_of(slot, me, experts)},
        )

    def forward(step, d):
        block = (rows.at[step, t], rows_pairs.at[step, t])
        return move(
            block, block, fwd_send.at[step, d], fwd_recv.at[step, d], {"tp": (t + d) % tps}
        )

    def share(step, d):
        dst = (t + d) % tps
        return move(
            (part.at[step, dst], part_pairs.at[step, dst]),
            (peer.at[step, d], peer_pairs.at[step, d]),
            part_send.at[step, d],
            part_recv.at[step, d],
            {"tp": dst},
        )

    def give_back(step):
        return move(
            (summed.at[step], summed_pairs.at[step]),
            (returned.at[me], returned_pairs.at[me]),
            ret_send.at[step],
            ret_recv.at[me],
            {"sp": source_of(step, me, experts)},
        )

    for step in dispatch_order(experts):
        dispatch(step).start()
    rows[0, t] = outgoing[me]
    if pairs:
        rows_pairs[0, t] = outgoing_pairs[me]
        returned[:, whole:] = jnp.zeros((experts, capacity - whole, width), jnp.bfloat16)

    def send_on(step):
        if step > 0:
            arrived(step).wait_recv()
        for d in range(1, tps):
            forward(step, d).start()

    def finish(step):
        for d in range(1, tps):
            share(step, d).wait_recv()
        total = part[step, t, :whole].astype(jnp.float32)
        for d in range(1, tps):
            total = total + peer[step, d, :whole].astype(jnp.float32)
        total = total.astype(jnp.bfloat16)
        rest = []
        for i in range(pairs):
            pair = part_pairs[step, t, i].astype(jnp.float32)
            for d in range(1, tps):
                pair = pair + peer_pairs[step, d, i].astype(jnp.float32)
            rest.append(pair.astype(jnp.bfloat16))
        if step == 0:
            returned[me, :whole] = total
        else:
            summed[step, :whole] = total
        for i in range(pairs):
            if step == 0:
                returned_pairs[me, i] = rest[i]
            else:
                summed_pairs[step, i] = rest[i]
        if step > 0:
            give_back(step).start()

    up_tile_width = gate_w.shape[1] // (2 if gate_w.shape[1] % 512 == 0 else 3)
    down_tile_width = width // 2
    hidden_width = gate_w.shape[1]

    def up_stage(k0, k1):
        m = (k1 - k0) * tps * capacity
        for step in range(k0, k1):
            for d in range(1, tps):
                forward(step, d).wait_recv()
            for side in range(tps):
                take_pairs(rows.at[step, side], rows_pairs.at[step, side])

        def up_tile(i, carry):
            cols = pl.ds(pl.multiple_of(i * up_tile_width, up_tile_width), up_tile_width)
            block = rows[k0:k1].reshape(m, width)
            gate = jnp.dot(block, gate_w[:, cols], preferred_element_type=jnp.float32)
            up = jnp.dot(block, up_w[:, cols], preferred_element_type=jnp.float32)
            hidden[:m, cols] = (gate / (1.0 + jnp.exp(-gate)) * up).astype(jnp.bfloat16)
            return carry

        lax.fori_loop(0, hidden_width // up_tile_width, up_tile, 0)

    def down_stage(k0, k1):
        m = (k1 - k0) * tps * capacity

        def down_tile(i, carry):
            cols = pl.ds(pl.multiple_of(i * down_tile_width, down_tile_width), down_tile_width)
            result = jnp.dot(hidden[:m], down_w[:, cols], preferred_element_type=jnp.float32)
            part[k0:k1, :, :, cols] = result.astype(jnp.bfloat16).reshape(
                k1 - k0, tps, capacity, down_tile_width
            )
            return carry

        lax.fori_loop(0, width // down_tile_width, down_tile, 0)
        for step in range(k0, k1):
            for side in range(tps):
                for i in range(pairs):
                    row = whole + 2 * i
                    part_pairs[step, side, i] = part[step, side, row : row + 2]

    waiting = {"U": weight_loads[:2], "D": weight_loads[2:]}
    for action, steps in order:
        for load in waiting.pop(action, ()):
            load.wait()
        with jax.named_scope(f"{action}{steps[0]}"):
            if action == "U":
                up_stage(steps[0], steps[-1] + 1)
            elif action == "D":
                down_stage(steps[0], steps[-1] + 1)
            else:
                for step in steps:
                    if action == "F":
                        send_on(step)
                    elif action == "G":
                        finish(step)
                    else:
                        for d in range(1, tps):
                            share(step, d).start()

    for d in range(1, experts):
        src = (me + d) % experts
        move(
            (summed.at[d], summed_pairs.at[d]),
            (returned.at[src], returned_pairs.at[src]),
            ret_send.at[d],
            ret_recv.at[src],
            {"sp": src},
        ).wait_recv()

    for e in range(experts):
        take_pairs(returned.at[e], returned_pairs.at[e])
    back = returned[...].reshape(lanes, width)
    across = (((0,), (0,)), ((), ()))
    moe_sum = lax.dot_general(combine_ref[0], back, across, preferred_element_type=jnp.float32)
    moe_sum = moe_sum + lax.dot_general(
        combine_ref[1], back, across, preferred_element_type=jnp.float32
    )
    pre_final = residual_scale * normed_ref[...].astype(jnp.float32) + moe_sum
    out_ref[...] = layer_norm(pre_final, gain_ref[...], bias_ref[...]).astype(jnp.bfloat16)

    for d in range(1, tps):
        for i in range(width // HEAD_TILE):
            head_copy(d, i, t, tps, head_part, head_peer, head_send, head_recv).wait_send()
    for step in range(experts):
        if step > 0:
            dispatch(step).wait_send()
            give_back(step).wait_send()
        for d in range(1, tps):
            forward(step, d).wait_send()
            share(step, d).wait_send()


def per_device(
    resid,
    queries,
    keys,
    values,
    doc_ids,
    sink_logits,
    out_proj,
    norm1_gain,
    norm1_bias,
    route_ids,
    route_weights,
    expert_gate,
    expert_up,
    expert_down,
    norm2_gain,
    norm2_bias,
):
    experts, tps = lax.axis_size("sp"), lax.axis_size("tp")
    toks, width = resid.shape
    tok_dev, kv_width = keys.shape
    capacity, _, pairs = split_rows(toks, experts)
    pairs = max(pairs, 1)
    order = work_order(experts)
    most = max(len(steps) for action, steps in order if action == "U")
    hidden_width = expert_gate.shape[2]
    reach = -(-(toks + 2 * WINDOW) // 128) * 128
    padded = (tps - 1) * toks + reach
    vmem = pl.BlockSpec(memory_space=pltpu.VMEM)
    hbm = pl.BlockSpec(memory_space=pltpu.HBM)
    bf16 = jnp.bfloat16
    dma = pltpu.SemaphoreType.DMA
    small = (
        queries,
        keys,
        values,
        doc_ids[None, :],
        sink_logits[None, :],
        norm1_gain[None, :],
        norm1_bias[None, :],
        route_ids.T,
        route_weights.T,
        norm2_gain[None, :],
        norm2_bias[None, :],
        resid,
        out_proj,
    )
    return pl.pallas_call(
        functools.partial(layer_kernel, experts, tps, order),
        out_shape=pltpu.VMEM((toks, width), bf16),
        in_specs=[hbm] * 16,
        out_specs=vmem,
        scratch_shapes=[pltpu.VMEM(a.shape, a.dtype) for a in small]
        + [
            pltpu.VMEM((padded, kv_width), bf16),
            pltpu.VMEM((padded, kv_width), bf16),
            pltpu.VMEM((2, 1, tok_dev), jnp.int32),
            pltpu.VMEM((tps, 1, reach), jnp.int32),
            pltpu.VMEM((tok_dev, 128), jnp.int32),
            pltpu.VMEM((toks, queries.shape[1]), bf16),
            pltpu.VMEM((tps, toks, width), bf16),
            pltpu.VMEM((tps, toks, width), bf16),
            pltpu.VMEM((toks, width), jnp.float32),
            pltpu.VMEM((toks, width), bf16),
            pltpu.VMEM((experts * capacity, toks), bf16),
            pltpu.VMEM((2, experts * capacity, toks), bf16),
            pltpu.VMEM((experts, capacity, width), bf16),
            pltpu.VMEM((experts, pairs, 2, width), bf16),
            pltpu.VMEM((experts, tps, capacity, width), bf16),
            pltpu.VMEM((experts, tps, pairs, 2, width), bf16),
            pltpu.VMEM((width, hidden_width), bf16),
            pltpu.VMEM((width, hidden_width), bf16),
            pltpu.VMEM((hidden_width, width), bf16),
            pltpu.VMEM((most * tps * capacity, hidden_width), bf16),
            pltpu.VMEM((experts, tps, capacity, width), bf16),
            pltpu.VMEM((experts, tps, pairs, 2, width), bf16),
            pltpu.VMEM((experts, tps, capacity, width), bf16),
            pltpu.VMEM((experts, tps, pairs, 2, width), bf16),
            pltpu.VMEM((experts, capacity, width), bf16),
            pltpu.VMEM((experts, pairs, 2, width), bf16),
            pltpu.VMEM((experts, capacity, width), bf16),
            pltpu.VMEM((experts, pairs, 2, width), bf16),
            dma((16,)),
            dma((experts, 2)),
            dma((experts, 2)),
            dma((experts, tps, 2)),
            dma((experts, tps, 2)),
            dma((experts, tps, 2)),
            dma((experts, tps, 2)),
            dma((experts, 2)),
            dma((experts, 2)),
            dma((6,)),
            dma((6,)),
            dma((tps, width // HEAD_TILE)),
            dma((tps, width // HEAD_TILE)),
        ],
        compiler_params=pltpu.CompilerParams(
            collective_id=0, has_side_effects=True, vmem_limit_bytes=VMEM_BYTES - 2 * toks * width
        ),
    )(*small, expert_gate, expert_up, expert_down)


def solution(mesh):
    return jax.shard_map(
        per_device,
        mesh=mesh,
        in_specs=(
            P(("grp", "sp", "tp"), None),
            P(("grp", "sp"), "tp"),
            P(("grp", "sp"), "tp"),
            P(("grp", "sp"), "tp"),
            P(("grp", "sp")),
            P("tp"),
            P("tp", None),
            P(),
            P(),
            P(("grp", "sp", "tp"), None),
            P(("grp", "sp", "tp"), None),
            P("sp", None, "tp"),
            P("sp", None, "tp"),
            P("sp", "tp", None),
            P(),
            P(),
        ),
        out_specs=P(("grp", "sp", "tp"), None),
        check_vma=False,
    )
```

```python
import functools

import jax
import jax.numpy as jnp
from jax import lax
from jax.experimental import pallas as pl
from jax.experimental.pallas import tpu as pltpu
from jax.sharding import PartitionSpec as P

HEAD_DIM = 64
WINDOW = 128
MESH = pl.DeviceIdType.MESH
CHUNKS = 4
HEAD_TILE = 512
VMEM_BYTES = 67043328


norm_epsilon = 1e-05
residual_scale = 1.4142135623730951
masked_score = -1e30


def layer_norm(values, gain_vec, bias_vec):
    mean_val = jnp.mean(values, -1, keepdims=True)
    centred = values - mean_val
    variance = jnp.mean(centred * centred, -1, keepdims=True)
    return centred * lax.rsqrt(variance + norm_epsilon) * gain_vec + bias_vec


def step_partner(step, sp_pos, count, back):
    chip, core = sp_pos // 2, sp_pos % 2
    half = count // 4
    side, place = chip // half, chip % half
    pair, flip = step // 2, step % 2
    if pair == 0:
        turn, cross = 0, False
    elif pair <= half:
        turn, cross = pair - 1, True
    else:
        turn, cross = pair - half, False
    target_side = 1 - side if cross else side
    move = half - turn if back else turn
    target = target_side * half + (place + move) % half
    return target * 2 + (core + flip) % 2


def chain_of_four(sp_pos):
    chip, core = sp_pos // 2, sp_pos % 2
    inner = chip * (3 - chip) // 2
    return chip, core, inner, chip + 1 - 2 * (chip % 2)


def target_of(step, sp_pos, count):
    if count != 8:
        return step_partner(step, sp_pos, count, False), step
    chip, core, inner, near = chain_of_four(sp_pos)
    pair, flip = step // 2, step % 2
    to = (chip, (chip + 2) % 4, 3 - chip, near)[pair]
    slot = (0, 1, 2 + inner, 3 + inner, 5, 6, 4 - 2 * inner, 7)[step]
    return to * 2 + (core + flip) % 2, slot


def source_of(slot, sp_pos, count):
    if count != 8:
        return step_partner(slot, sp_pos, count, True)
    chip, core, inner, near = chain_of_four(sp_pos)
    even, far = (chip + 2) % 4, 3 - chip
    middle, end = (
        ((chip, 0), (chip, 0)),
        ((chip, 1), (chip, 1)),
        ((even, 0), (near, 0)),
        ((even, 1), (even, 0)),
        ((near, 0), (even, 1)),
        ((far, 0), (far, 0)),
        ((far, 1), (far, 1)),
        ((near, 1), (near, 1)),
    )[slot]
    of, flip = (inner * m + (1 - inner) * e for m, e in zip(middle, end))
    return of * 2 + (core + flip) % 2


def dispatch_order(count):
    return (1, 2, 3, 6, 7, 4, 5) if count == 8 else range(1, count)


def work_order(count):
    if count == 8:
        return [
            ("F", (0,)),
            ("F", (1,)),
            ("F", (2,)),
            ("U", (0, 1,)),
            ("F", (3,)),
            ("D", (0, 1,)),
            ("U", (2,)),
            ("F", (4,)),
            ("D", (2,)),
            ("X", (2,)),
            ("U", (3,)),
            ("F", (7,)),
            ("D", (3,)),
            ("U", (4,)),
            ("F", (5,)),
            ("X", (3,)),
            ("D", (4,)),
            ("U", (7,)),
            ("F", (6,)),
            ("X", (4,)),
            ("G", (2,)),
            ("D", (7,)),
            ("U", (5,)),
            ("G", (3,)),
            ("D", (5,)),
            ("X", (5,)),
            ("U", (6,)),
            ("G", (4,)),
            ("D", (6,)),
            ("X", (6,)),
            ("X", (7,)),
            ("X", (0,)),
            ("X", (1,)),
            ("G", (5,)),
            ("G", (6,)),
            ("G", (7,)),
            ("G", (0,)),
            ("G", (1,)),
        ]
    chunk = count // CHUNKS
    groups = [tuple(range(c * chunk, (c + 1) * chunk)) for c in range(CHUNKS)]
    order = [("F", groups[0])]
    for c, group in enumerate(groups):
        order.append(("U", group))
        if c + 1 < CHUNKS:
            order.append(("F", groups[c + 1]))
        order += [("D", group), ("X", group)]
        if c > 0:
            order.append(("G", groups[c - 1]))
    return order + [("G", groups[-1])]


def split_rows(toks, experts):
    need = 5 * toks // (2 * experts)
    whole, pairs = need // 8 * 8, -(-(need % 8) // 2)
    if whole == 0 or pairs in (0, 4):
        whole, pairs = -(-need // 16) * 16, 0
    return -(-need // 16) * 16, whole, pairs


class Copies:
    def __init__(self, source, target, send, recv, device, whole, pairs):
        ends = [(source[0].at[pl.ds(0, whole)], target[0].at[pl.ds(0, whole)])]
        if pairs:
            ends.append((source[1], target[1]))
        self.copies = [
            pltpu.make_async_remote_copy(
                src_ref=src,
                dst_ref=dst,
                send_sem=send.at[i],
                recv_sem=recv.at[i],
                device_id=device,
                device_id_type=MESH,
            )
            for i, (src, dst) in enumerate(ends)
        ]

    def start(self):
        for copy in self.copies:
            copy.start()

    def wait_recv(self):
        for copy in self.copies:
            copy.wait_recv()

    def wait_send(self):
        for copy in self.copies:
            copy.wait_send()


def head_copy(d, i, t, tps, head_part, head_peer, head_send, head_recv):
    cols = pl.ds(pl.multiple_of(i * HEAD_TILE, HEAD_TILE), HEAD_TILE)
    return pltpu.make_async_remote_copy(
        src_ref=head_part.at[d, :, cols],
        dst_ref=head_peer.at[d, :, cols],
        send_sem=head_send.at[d, i],
        recv_sem=head_recv.at[d, i],
        device_id={"tp": (t + d) % tps},
        device_id_type=MESH,
    )


def attend(
    count,
    tps,
    queries_ref,
    keys_ref,
    values_ref,
    docs_ref,
    sink_ref,
    proj_w,
    key_pad,
    value_pad,
    doc_side,
    doc_rows,
    doc_cols,
    attended,
    head_part,
    head_peer,
    halo_send,
    halo_recv,
    head_send,
    head_recv,
    barrier,
    kv_copies,
    query_copies,
    proj_copy,
):
    me, t = lax.axis_index("sp"), lax.axis_index("tp")
    tok_dev, tok_sub = queries_ref.shape[0], attended.shape[0]
    local_kv = keys_ref.shape[1] // HEAD_DIM
    heads = queries_ref.shape[1] // HEAD_DIM
    groups = heads // local_kv
    reach = doc_rows.shape[2]
    end = WINDOW + tok_dev
    rest = key_pad.shape[0] - end - WINDOW
    for copy in kv_copies:
        copy.wait()
    pl.semaphore_wait(barrier, count - 1 + tps - 1)
    copies = []
    for side in range(2):
        start, place = (tok_dev - WINDOW, 0) if side == 0 else (0, end)
        to = (me + 1) % count if side == 0 else (me + count - 1) % count
        pairs = (
            (keys_ref.at[pl.ds(start, WINDOW)], key_pad.at[pl.ds(place, WINDOW)]),
            (values_ref.at[pl.ds(start, WINDOW)], value_pad.at[pl.ds(place, WINDOW)]),
            (docs_ref, doc_side.at[side]),
        )
        for i, (own, pad) in enumerate(pairs):
            copies.append(
                pltpu.make_async_remote_copy(
                    src_ref=own,
                    dst_ref=pad,
                    send_sem=halo_send.at[2 * i + side],
                    recv_sem=halo_recv.at[2 * i + side],
                    device_id={"sp": to},
                    device_id_type=MESH,
                )
            )
    for copy in copies:
        copy.start()
    for pad, own in ((key_pad, keys_ref), (value_pad, values_ref)):
        pad[WINDOW:end] = own[...]
        if rest:
            pad[end + WINDOW :] = jnp.zeros((rest, pad.shape[1]), pad.dtype)
    doc_cols[...] = jnp.transpose(jnp.broadcast_to(docs_ref[...], (128, tok_dev)))
    for copy in query_copies:
        copy.wait()
    for copy in copies:
        copy.wait_recv()
    doc_row = jnp.concatenate(
        [doc_side[0][:, tok_dev - WINDOW :], docs_ref[...], doc_side[1][:, :WINDOW]]
        + ([jnp.zeros((1, rest), jnp.int32)] if rest else []),
        1,
    )
    for j in range(tps):
        doc_rows[j] = doc_row[:, j * tok_sub : j * tok_sub + reach]

    tile = HEAD_TILE
    width = proj_w.shape[1]
    for d in list(range(1, tps)) + [0]:
        block = (t + d) % tps
        base = pl.multiple_of(block * tok_sub, 16)
        key_block = key_pad[pl.ds(base, reach), :].astype(jnp.float32)
        value_block = value_pad[pl.ds(base, reach), :].astype(jnp.float32)
        key_docs = doc_rows[block]
        query_docs = doc_cols[pl.ds(base, tok_sub), 0:1]
        row = lax.broadcasted_iota(jnp.int32, (tok_sub, reach), 0)
        col = lax.broadcasted_iota(jnp.int32, (tok_sub, reach), 1)
        position = me * tok_dev + base - WINDOW + col
        allowed = (position >= 0) & (position < count * tok_dev)
        allowed = allowed & (col >= row) & (col <= row + 2 * WINDOW)
        allowed = allowed & (query_docs == key_docs)
        bias = jnp.where(allowed, 0.0, masked_score)
        low = lax.broadcasted_iota(jnp.int32, (1, 2 * HEAD_DIM), 1) < HEAD_DIM
        pairs = groups // 2
        for g in range(local_kv):
            span = slice(g // 2 * 2 * HEAD_DIM, g // 2 * 2 * HEAD_DIM + 2 * HEAD_DIM)
            key_side, value_side = key_block[:, span], value_block[:, span]
            if key_side.shape[1] < 2 * HEAD_DIM:
                blank = jnp.zeros((reach, HEAD_DIM), jnp.float32)
                key_side = jnp.concatenate([key_side, blank], 1)
                value_side = jnp.concatenate([value_side, blank], 1)
            here = low if g % 2 == 0 else jnp.logical_not(low)
            key_side = jnp.where(here, key_side, 0.0).astype(jnp.bfloat16)
            value_side = jnp.where(here, value_side, 1.0).astype(jnp.bfloat16)
            first = g * groups
            query = [
                queries_ref[
                    pl.ds(base, tok_sub),
                    (first + 2 * p) * HEAD_DIM : (first + 2 * p + 2) * HEAD_DIM,
                ].astype(jnp.float32)
                * HEAD_DIM ** (-0.5)
                for p in range(pairs)
            ]
            ratios = []
            for parity in range(2):
                turned = parity != g % 2
                stack = jnp.concatenate(
                    [pltpu.roll(q, HEAD_DIM, 1) if turned else q for q in query], 0
                ).astype(jnp.bfloat16)
                scores = lax.dot_general(
                    stack, key_side, (((1,), (1,)), ((), ())), preferred_element_type=jnp.float32
                )
                weights, sinks = [], []
                for p in range(pairs):
                    head = first + 2 * p + parity
                    sink = sink_ref[:, head : head + 1]
                    score = scores[p * tok_sub : (p + 1) * tok_sub] + bias
                    top = jnp.maximum(jnp.max(score, -1, keepdims=True), sink)
                    weights.append(jnp.exp(score - top).astype(jnp.bfloat16))
                    sinks.append(jnp.exp(sink - top))
                result = jnp.dot(
                    jnp.concatenate(weights, 0), value_side, preferred_element_type=jnp.float32
                )
                other = pltpu.roll(result, HEAD_DIM, 1)
                top_side, sum_side = (other, result) if turned else (result, other)
                ratios.append(top_side / (sum_side + jnp.concatenate(sinks, 0)))
            joined = jnp.where(low, ratios[0], ratios[1]).astype(jnp.bfloat16)
            for p in range(pairs):
                lane = (first + 2 * p) * HEAD_DIM
                attended[:, lane : lane + 2 * HEAD_DIM] = joined[p * tok_sub : (p + 1) * tok_sub]
        if d == 1 or tps == 1:
            proj_copy.wait()

        def project(i, carry):
            cols = pl.ds(pl.multiple_of(i * tile, tile), tile)
            head_part[d, :, cols] = jnp.dot(
                attended[...], proj_w[:, cols], preferred_element_type=jnp.float32
            ).astype(jnp.bfloat16)
            if d:
                head_copy(d, i, t, tps, head_part, head_peer, head_send, head_recv).start()
            return carry

        lax.fori_loop(0, width // tile, project, 0)
    for copy in copies:
        copy.wait_send()


def layer_kernel(
    experts,
    tps,
    order,
    queries_hbm,
    keys_hbm,
    values_hbm,
    docs_hbm,
    sink_hbm,
    gain1_hbm,
    bias1_hbm,
    ids_hbm,
    mix_hbm,
    gain_hbm,
    bias_hbm,
    resid_hbm,
    proj_hbm,
    gate_hbm,
    up_hbm,
    down_hbm,
    out_ref,
    queries_ref,
    keys_ref,
    values_ref,
    docs_ref,
    sink_ref,
    gain1_ref,
    bias1_ref,
    ids_ref,
    mix_ref,
    gain_ref,
    bias_ref,
    resid_ref,
    proj_w,
    key_pad,
    value_pad,
    doc_side,
    doc_rows,
    doc_cols,
    attended,
    head_part,
    head_peer,
    pre_ref,
    normed_ref,
    assign_ref,
    combine_ref,
    outgoing,
    outgoing_pairs,
    rows,
    rows_pairs,
    gate_w,
    up_w,
    down_w,
    hidden,
    part,
    part_pairs,
    peer,
    peer_pairs,
    summed,
    summed_pairs,
    returned,
    returned_pairs,
    in_sem,
    disp_send,
    disp_recv,
    fwd_send,
    fwd_recv,
    part_send,
    part_recv,
    ret_send,
    ret_recv,
    halo_send,
    halo_recv,
    head_send,
    head_recv,
):
    me, t = lax.axis_index("sp"), lax.axis_index("tp")
    width = outgoing.shape[2]
    toks = normed_ref.shape[0]
    capacity, whole, pairs = split_rows(toks, experts)

    def take_pairs(block, block_pairs):
        for i in range(pairs):
            block[whole + 2 * i : whole + 2 * i + 2] = block_pairs[i]


    barrier = pltpu.get_barrier_semaphore()
    for d in range(1, experts):
        pl.semaphore_signal(
            barrier, inc=1, device_id={"sp": (me + d) % experts}, device_id_type=MESH
        )
    for d in range(1, tps):
        pl.semaphore_signal(barrier, inc=1, device_id={"tp": (t + d) % tps}, device_id_type=MESH)

    places = (
        (keys_hbm, keys_ref),
        (values_hbm, values_ref),
        (docs_hbm, docs_ref),
        (queries_hbm, queries_ref),
        (sink_hbm, sink_ref),
        (proj_hbm, proj_w),
        (ids_hbm, ids_ref),
        (mix_hbm, mix_ref),
        (resid_hbm, resid_ref),
        (gain1_hbm, gain1_ref),
        (bias1_hbm, bias1_ref),
        (gain_hbm, gain_ref),
        (bias_hbm, bias_ref),
        (gate_hbm.at[0], gate_w),
        (up_hbm.at[0], up_w),
        (down_hbm.at[0], down_w),
    )
    loads = [
        pltpu.make_async_copy(source, place, in_sem.at[i])
        for i, (source, place) in enumerate(places)
    ]
    for load in loads:
        load.start()
    weight_loads = loads[13:]

    attend(
        experts,
        tps,
        queries_ref,
        keys_ref,
        values_ref,
        docs_ref,
        sink_ref,
        proj_w,
        key_pad,
        value_pad,
        doc_side,
        doc_rows,
        doc_cols,
        attended,
        head_part,
        head_peer,
        halo_send,
        halo_recv,
        head_send,
        head_recv,
        barrier,
        loads[:3],
        loads[3:5],
        loads[5],
    )
    for load in loads[6:13]:
        load.wait()
    lanes = experts * capacity
    top = ids_ref.shape[0]
    expert_iota = lax.broadcasted_iota(jnp.int32, (experts, toks), 0)
    upper = (
        lax.broadcasted_iota(jnp.int32, (toks, toks), 0)
        < lax.broadcasted_iota(jnp.int32, (toks, toks), 1)
    ).astype(jnp.float32).astype(jnp.bfloat16)
    before = jnp.zeros((experts, 1), jnp.float32)
    slot_iota = lax.broadcasted_iota(jnp.int32, (lanes, toks), 0)
    assign = jnp.zeros((lanes, toks), jnp.float32)
    combine = jnp.zeros((lanes, toks), jnp.float32)
    for k in range(top):
        own = ids_ref[k : k + 1, :]
        hot = (own == expert_iota).astype(jnp.float32)
        rank = before + jnp.dot(hot.astype(jnp.bfloat16), upper, preferred_element_type=jnp.float32)
        rank = jnp.sum(rank * hot, axis=0, keepdims=True).astype(jnp.int32)
        before = before + jnp.sum(hot, axis=1, keepdims=True)
        match = (own * capacity + rank == slot_iota).astype(jnp.float32)
        assign = assign + match
        combine = combine + match * mix_ref[k : k + 1, :]
    assign_ref[...] = assign.astype(jnp.bfloat16)
    high = combine.astype(jnp.bfloat16)
    combine_ref[0] = high
    combine_ref[1] = (combine - high.astype(jnp.float32)).astype(jnp.bfloat16)

    total = jnp.zeros((toks, 1), jnp.float32)
    for i in range(width // HEAD_TILE):
        cols = slice(i * HEAD_TILE, (i + 1) * HEAD_TILE)
        projected = head_part[0, :, cols].astype(jnp.float32)
        for d in range(1, tps):
            head_copy(d, i, t, tps, head_part, head_peer, head_send, head_recv).wait_recv()
            projected = projected + head_peer[d, :, cols].astype(jnp.float32)
        projected = projected.astype(jnp.bfloat16).astype(jnp.float32)
        pre_norm = residual_scale * resid_ref[:, cols].astype(jnp.float32) + projected
        pre_ref[:, cols] = pre_norm
        total = total + jnp.sum(pre_norm, -1, keepdims=True)
    centred = pre_ref[...] - total * (1.0 / width)
    variance = jnp.mean(centred * centred, -1, keepdims=True)
    normed = centred * lax.rsqrt(variance + norm_epsilon) * gain1_ref[...] + bias1_ref[...]
    normed_ref[...] = normed.astype(jnp.bfloat16)
    spread = jnp.dot(assign_ref[...], normed_ref[...], preferred_element_type=jnp.float32)
    outgoing[...] = spread.astype(jnp.bfloat16).reshape(experts, capacity, width)
    for e in range(experts):
        for i in range(pairs):
            row = whole + 2 * i
            outgoing_pairs[e, i] = outgoing[e, row : row + 2]

    def move(source, target, send, recv, device):
        return Copies(source, target, send, recv, device, whole, pairs)

    def dispatch(step):
        dst, slot = target_of(step, me, experts)
        return move(
            (outgoing.at[dst], outgoing_pairs.at[dst]),
            (rows.at[slot, t], rows_pairs.at[slot, t]),
            disp_send.at[step],
            disp_recv.at[slot],
            {"sp": dst},
        )

    def arrived(slot):
        return move(
            (outgoing.at[slot], outgoing_pairs.at[slot]),
            (rows.at[slot, t], rows_pairs.at[slot, t]),
            disp_send.at[slot],
            disp_recv.at[slot],
            {"sp": source_of(slot, me, experts)},
        )

    def forward(step, d):
        block = (rows.at[step, t], rows_pairs.at[step, t])
        return move(
            block, block, fwd_send.at[step, d], fwd_recv.at[step, d], {"tp": (t + d) % tps}
        )

    def share(step, d):
        dst = (t + d) % tps
        return move(
            (part.at[step, dst], part_pairs.at[step, dst]),
            (peer.at[step, d], peer_pairs.at[step, d]),
            part_send.at[step, d],
            part_recv.at[step, d],
            {"tp": dst},
        )

    def give_back(step):
        return move(
            (summed.at[step], summed_pairs.at[step]),
            (returned.at[me], returned_pairs.at[me]),
            ret_send.at[step],
            ret_recv.at[me],
            {"sp": source_of(step, me, experts)},
        )

    for step in dispatch_order(experts):
        dispatch(step).start()
    rows[0, t] = outgoing[me]
    if pairs:
        rows_pairs[0, t] = outgoing_pairs[me]
        returned[:, whole:] = jnp.zeros((experts, capacity - whole, width), jnp.bfloat16)

    def send_on(step):
        if step > 0:
            arrived(step).wait_recv()
        for d in range(1, tps):
            forward(step, d).start()

    def finish(step):
        for d in range(1, tps):
            share(step, d).wait_recv()
        total = part[step, t, :whole].astype(jnp.float32)
        for d in range(1, tps):
            total = total + peer[step, d, :whole].astype(jnp.float32)
        total = total.astype(jnp.bfloat16)
        rest = []
        for i in range(pairs):
            pair = part_pairs[step, t, i].astype(jnp.float32)
            for d in range(1, tps):
                pair = pair + peer_pairs[step, d, i].astype(jnp.float32)
            rest.append(pair.astype(jnp.bfloat16))
        if step == 0:
            returned[me, :whole] = total
        else:
            summed[step, :whole] = total
        for i in range(pairs):
            if step == 0:
                returned_pairs[me, i] = rest[i]
            else:
                summed_pairs[step, i] = rest[i]
        if step > 0:
            give_back(step).start()

    up_tile_width = gate_w.shape[1] // (2 if gate_w.shape[1] % 512 == 0 else 3)
    down_tile_width = width // 2
    hidden_width = gate_w.shape[1]

    def up_stage(k0, k1):
        m = (k1 - k0) * tps * capacity
        for step in range(k0, k1):
            for d in range(1, tps):
                forward(step, d).wait_recv()
            for side in range(tps):
                take_pairs(rows.at[step, side], rows_pairs.at[step, side])

        def up_tile(i, carry):
            cols = pl.ds(pl.multiple_of(i * up_tile_width, up_tile_width), up_tile_width)
            block = rows[k0:k1].reshape(m, width)
            gate = jnp.dot(block, gate_w[:, cols], preferred_element_type=jnp.float32)
            up = jnp.dot(block, up_w[:, cols], preferred_element_type=jnp.float32)
            hidden[:m, cols] = (gate / (1.0 + jnp.exp(-gate)) * up).astype(jnp.bfloat16)
            return carry

        lax.fori_loop(0, hidden_width // up_tile_width, up_tile, 0)

    def down_stage(k0, k1):
        m = (k1 - k0) * tps * capacity

        def down_tile(i, carry):
            cols = pl.ds(pl.multiple_of(i * down_tile_width, down_tile_width), down_tile_width)
            result = jnp.dot(hidden[:m], down_w[:, cols], preferred_element_type=jnp.float32)
            part[k0:k1, :, :, cols] = result.astype(jnp.bfloat16).reshape(
                k1 - k0, tps, capacity, down_tile_width
            )
            return carry

        lax.fori_loop(0, width // down_tile_width, down_tile, 0)
        for step in range(k0, k1):
            for side in range(tps):
                for i in range(pairs):
                    row = whole + 2 * i
                    part_pairs[step, side, i] = part[step, side, row : row + 2]

    waiting = {"U": weight_loads[:2], "D": weight_loads[2:]}
    for action, steps in order:
        for load in waiting.pop(action, ()):
            load.wait()
        with jax.named_scope(f"{action}{steps[0]}"):
            if action == "U":
                up_stage(steps[0], steps[-1] + 1)
            elif action == "D":
                down_stage(steps[0], steps[-1] + 1)
            else:
                for step in steps:
                    if action == "F":
                        send_on(step)
                    elif action == "G":
                        finish(step)
                    else:
                        for d in range(1, tps):
                            share(step, d).start()

    for d in range(1, experts):
        src = (me + d) % experts
        move(
            (summed.at[d], summed_pairs.at[d]),
            (returned.at[src], returned_pairs.at[src]),
            ret_send.at[d],
            ret_recv.at[src],
            {"sp": src},
        ).wait_recv()

    for e in range(experts):
        take_pairs(returned.at[e], returned_pairs.at[e])
    back = returned[...].reshape(lanes, width)
    across = (((0,), (0,)), ((), ()))
    moe_sum = lax.dot_general(combine_ref[0], back, across, preferred_element_type=jnp.float32)
    moe_sum = moe_sum + lax.dot_general(
        combine_ref[1], back, across, preferred_element_type=jnp.float32
    )
    pre_final = residual_scale * normed_ref[...].astype(jnp.float32) + moe_sum
    out_ref[...] = layer_norm(pre_final, gain_ref[...], bias_ref[...]).astype(jnp.bfloat16)

    for d in range(1, tps):
        for i in range(width // HEAD_TILE):
            head_copy(d, i, t, tps, head_part, head_peer, head_send, head_recv).wait_send()
    for step in range(experts):
        if step > 0:
            dispatch(step).wait_send()
            give_back(step).wait_send()
        for d in range(1, tps):
            forward(step, d).wait_send()
            share(step, d).wait_send()


def per_device(
    resid,
    queries,
    keys,
    values,
    doc_ids,
    sink_logits,
    out_proj,
    norm1_gain,
    norm1_bias,
    route_ids,
    route_weights,
    expert_gate,
    expert_up,
    expert_down,
    norm2_gain,
    norm2_bias,
):
    experts, tps = lax.axis_size("sp"), lax.axis_size("tp")
    toks, width = resid.shape
    tok_dev, kv_width = keys.shape
    capacity, _, pairs = split_rows(toks, experts)
    pairs = max(pairs, 1)
    order = work_order(experts)
    most = max(len(steps) for action, steps in order if action == "U")
    hidden_width = expert_gate.shape[2]
    reach = -(-(toks + 2 * WINDOW) // 128) * 128
    padded = (tps - 1) * toks + reach
    vmem = pl.BlockSpec(memory_space=pltpu.VMEM)
    hbm = pl.BlockSpec(memory_space=pltpu.HBM)
    bf16 = jnp.bfloat16
    dma = pltpu.SemaphoreType.DMA
    small = (
        queries,
        keys,
        values,
        doc_ids[None, :],
        sink_logits[None, :],
        norm1_gain[None, :],
        norm1_bias[None, :],
        route_ids.T,
        route_weights.T,
        norm2_gain[None, :],
        norm2_bias[None, :],
        resid,
        out_proj,
    )
    return pl.pallas_call(
        functools.partial(layer_kernel, experts, tps, order),
        out_shape=pltpu.VMEM((toks, width), bf16),
        in_specs=[hbm] * 16,
        out_specs=vmem,
        scratch_shapes=[pltpu.VMEM(a.shape, a.dtype) for a in small]
        + [
            pltpu.VMEM((padded, kv_width), bf16),
            pltpu.VMEM((padded, kv_width), bf16),
            pltpu.VMEM((2, 1, tok_dev), jnp.int32),
            pltpu.VMEM((tps, 1, reach), jnp.int32),
            pltpu.VMEM((tok_dev, 128), jnp.int32),
            pltpu.VMEM((toks, queries.shape[1]), bf16),
            pltpu.VMEM((tps, toks, width), bf16),
            pltpu.VMEM((tps, toks, width), bf16),
            pltpu.VMEM((toks, width), jnp.float32),
            pltpu.VMEM((toks, width), bf16),
            pltpu.VMEM((experts * capacity, toks), bf16),
            pltpu.VMEM((2, experts * capacity, toks), bf16),
            pltpu.VMEM((experts, capacity, width), bf16),
            pltpu.VMEM((experts, pairs, 2, width), bf16),
            pltpu.VMEM((experts, tps, capacity, width), bf16),
            pltpu.VMEM((experts, tps, pairs, 2, width), bf16),
            pltpu.VMEM((width, hidden_width), bf16),
            pltpu.VMEM((width, hidden_width), bf16),
            pltpu.VMEM((hidden_width, width), bf16),
            pltpu.VMEM((most * tps * capacity, hidden_width), bf16),
            pltpu.VMEM((experts, tps, capacity, width), bf16),
            pltpu.VMEM((experts, tps, pairs, 2, width), bf16),
            pltpu.VMEM((experts, tps, capacity, width), bf16),
            pltpu.VMEM((experts, tps, pairs, 2, width), bf16),
            pltpu.VMEM((experts, capacity, width), bf16),
            pltpu.VMEM((experts, pairs, 2, width), bf16),
            pltpu.VMEM((experts, capacity, width), bf16),
            pltpu.VMEM((experts, pairs, 2, width), bf16),
            dma((16,)),
            dma((experts, 2)),
            dma((experts, 2)),
            dma((experts, tps, 2)),
            dma((experts, tps, 2)),
            dma((experts, tps, 2)),
            dma((experts, tps, 2)),
            dma((experts, 2)),
            dma((experts, 2)),
            dma((6,)),
            dma((6,)),
            dma((tps, width // HEAD_TILE)),
            dma((tps, width // HEAD_TILE)),
        ],
        compiler_params=pltpu.CompilerParams(
            collective_id=0, has_side_effects=True, vmem_limit_bytes=VMEM_BYTES - 2 * toks * width
        ),
    )(*small, expert_gate, expert_up, expert_down)


def solution(mesh):
    return jax.shard_map(
        per_device,
        mesh=mesh,
        in_specs=(
            P(("grp", "sp", "tp"), None),
            P(("grp", "sp"), "tp"),
            P(("grp", "sp"), "tp"),
            P(("grp", "sp"), "tp"),
            P(("grp", "sp")),
            P("tp"),
            P("tp", None),
            P(),
            P(),
            P(("grp", "sp", "tp"), None),
            P(("grp", "sp", "tp"), None),
            P("sp", None, "tp"),
            P("sp", None, "tp"),
            P("sp", "tp", None),
            P(),
            P(),
        ),
        out_specs=P(("grp", "sp", "tp"), None),
        check_vma=False,
    )
```
